256 devices in a mesh: sp: 16 (over y, x), tp: 16 (over z, core).
Axes of the slice: x: 4, y: 4, z: 8, core: 2. Of those that a mesh axis runs over, the one named last changes fastest.
Arguments:
- conv_value: bfloat16 [49152, 2048], P('sp', 'tp'), may hold values from -48 to 48
- conv_gate: bfloat16 [49152, 2048], P('sp', 'tp'), may hold values from -6 to 6
- doc_ids: int32 [49152], P('sp'), may hold values from 0 to 15, never falling along the last dimension, each value on 1 to 9216 neighbouring positions
- conv_kernel: bfloat16 [31, 2048], P(None, 'tp'), may hold values from -1 to 1
- norm_gain_conv: float32 [2048], replicated, may hold values from 0.1 to 1.9
- norm_bias_conv: float32 [2048], replicated, may hold values from -3 to 3
- proj_weight: bfloat16 [2048, 2048], P('tp'), may hold values from -0.125 to 0.125
- residual: bfloat16 [49152, 2048], P(('sp', 'tp')), may hold values from -6 to 6
- norm_gain_moe: float32 [2048], replicated, may hold values from 0.1 to 1.9
- group_router: bfloat16 [2048, 2], replicated, may hold values from -0.125 to 0.125
- expert_router: bfloat16 [2048, 16], replicated, may hold values from -0.125 to 0.125
- routing: int32 [49152, 2], P(('sp', 'tp')), may hold values from 0 to 15, as said below
- expert_gate_w: bfloat16 [16, 2048, 512], P('sp'), may hold values from -0.125 to 0.125
- expert_up_w: bfloat16 [16, 2048, 512], P('sp'), may hold values from -0.125 to 0.125
- expert_down_w: bfloat16 [16, 512, 2048], P('sp'), may hold values from -0.25 to 0.25
Outputs:
- output: bfloat16 [49152, 2048], P(('sp', 'tp'))
The draws below stay inside these ranges and needn't reach their ends.
Inputs may be any that keep to these rules, and one draw needn't show every extreme that they name: `routing`: both numbers of a row are different experts of one group (expert // 8); within the rows of one device (aligned blocks of 192 rows) every expert is named exactly 24 times.
All inputs are finite; a program needn't handle non-finite values.
Results may differ from the reference program's by a relative error of at most 0.015.
Values may be sent and summed in bfloat16 or wider, within the bound.
No kernel may reach another device: no remote copies, remote signals or barrier semaphores. Data moves between devices by JAX's collectives and lax.ppermute only.
A program may use at most 64 MiB of HBM per device.

```python
import math
import jax
import jax.numpy as jnp
import numpy as np
from jax import lax

D = 2048
CH = 2048
KW = 31
FF = 512
GROUPS = 2
TOK_DEV = 192
EXPERTS = 16
TOKENS = 49152
DOCS = 16
DOC_MOST = 9216


def draw_conv_value(key, part):
    base_key = jax.random.fold_in(key, 101)
    column_key = jax.random.fold_in(key, 102)
    column_scale = 3.0 ** (jnp.arange(CH, dtype=jnp.float32) / CH) * jax.random.uniform(column_key, (CH,), jnp.float32, 0.6, 1.6)
    base = jnp.clip(jax.random.normal(base_key, (TOKENS, CH), jnp.float32), -6.0, 6.0)
    return (base * column_scale[None, :]).astype(jnp.bfloat16)


def draw_routing(key, part):
    blocks = TOKENS // TOK_DEV
    per_group = EXPERTS // GROUPS
    group_rows = TOK_DEV // GROUPS
    per_expert = TOK_DEV // EXPERTS
    shift_key = jax.random.fold_in(key, 201)
    flip_key = jax.random.fold_in(key, 202)
    shuffle_key = jax.random.fold_in(key, 203)
    rank_order = jnp.arange(TOK_DEV, dtype=jnp.int32)
    first_local = rank_order % group_rows // per_expert
    shifts = jax.random.randint(shift_key, (blocks,), 1, per_group, jnp.int32)
    flips = jax.random.randint(flip_key, (blocks,), 0, GROUPS, jnp.int32)
    group_index = (rank_order[None, :] // group_rows + flips[:, None]) % GROUPS
    second_local = (first_local[None, :] + shifts[:, None]) % per_group
    first_expert = group_index * per_group + first_local[None, :]
    second_expert = group_index * per_group + second_local
    pairing = jnp.stack([first_expert, second_expert], axis=-1).astype(jnp.int32)
    shuffles = jax.vmap(lambda block_key: jax.random.permutation(block_key, TOK_DEV))(jax.random.split(shuffle_key, blocks))

    def place_block(shuffle, block_pairs):
        return jnp.zeros((TOK_DEV, 2), jnp.int32).at[shuffle].set(block_pairs)
    routed = jax.vmap(place_block)(shuffles.astype(jnp.int32), pairing)
    return routed.reshape(TOKENS, 2).astype(jnp.int32)


def shard_levels(key, dims, cuts, smallest, high):
    loudness, own = 1.0, jax.random.fold_in(key, 6)
    for axis_at, shards_of in cuts:
        steps = jnp.exp(jax.random.uniform(jax.random.fold_in(own, axis_at), (shards_of,), jnp.float32, smallest / len(cuts), high / len(cuts)))
        loudness = loudness * jnp.repeat(steps, dims[axis_at] // shards_of).reshape([-1 if axis == axis_at else 1 for axis in range(len(dims))])
    return loudness


def length_profile(count, total, reach, lean):
    portions = [(1 << 20) // math.isqrt(grade ** lean) + 1 for grade in range(2, count + 1)]
    surplus, given = total - reach - (count - 1), [1] * (count - 1)
    while surplus > 0:
        movable = [i for i in range(count - 1) if given[i] < reach]
        mass, budget = sum([portions[i] for i in movable]), surplus
        for i in movable:
            more = min(reach - given[i], max(1, budget * portions[i] // mass), surplus)
            given[i] = given[i] + more
            surplus = surplus - more
    return np.array([reach] + given)


def ragged_sizes(rng, number_of, total, limit, skew):
    if number_of == 2:
        one = jax.random.randint(rng, (), max(1, total - limit), min(limit, total - 1) + 1)
        return jnp.stack([one, total - one])
    tallies = jnp.asarray(length_profile(number_of, total, limit, skew), jnp.int32)
    couples = (number_of - 1) // 2
    donor, taker = tallies[1:1 + 2 * couples:2], tallies[2:2 + 2 * couples:2]
    room = jnp.minimum(donor - 1, limit - taker)
    moved = jax.random.randint(jax.random.fold_in(rng, 1), (couples,), 0, 1 << 20) % (room + 1)
    tallies = tallies.at[1:1 + 2 * couples:2].set(donor - moved).at[2:2 + 2 * couples:2].set(taker + moved)
    return tallies[jax.random.permutation(jax.random.fold_in(rng, 2), number_of)]


def normal_values(key, extent, spread, limit, cuts=(), kind=jnp.bfloat16):
    array = jax.random.normal(key, extent, jnp.float32) * spread
    if len(cuts) > 0:
        array = shard_levels(key, extent, cuts, -0.22, 0.18) * array
    return jnp.clip(array, min=-limit, max=limit).astype(kind)


def setup_inputs(seed: int = 0) -> dict:
    seeds = jax.random.split(jax.random.key(seed), 16)
    return {
        "conv_value": draw_conv_value(jax.random.fold_in(seeds[15], 71), 0),
        "conv_gate": normal_values(seeds[1], (TOKENS, CH), 1.0, 6.0, ((0, 16), (1, 16))),
        "doc_ids": jnp.searchsorted(jnp.cumsum(ragged_sizes(seeds[2], DOCS, TOKENS, DOC_MOST, 0)), jnp.arange(TOKENS), side="right").astype(jnp.int32),
        "conv_kernel": normal_values(seeds[3], (KW, CH), KW ** -0.5, 1.0, ((1, 16),)),
        "norm_gain_conv": jnp.clip(1.0 + 0.18 * jax.random.normal(seeds[4], (CH,), jnp.float32), 0.1, 1.9),
        "norm_bias_conv": normal_values(seeds[5], (CH,), 0.5, 3.0, (), jnp.float32),
        "proj_weight": normal_values(seeds[6], (CH, D), CH ** -0.5, 0.125, ((0, 16),)),
        "residual": normal_values(seeds[7], (TOKENS, D), 1.0, 6.0, ((0, 256),)),
        "norm_gain_moe": jnp.clip(1.0 + 0.18 * jax.random.normal(seeds[8], (D,), jnp.float32), 0.1, 1.9),
        "group_router": normal_values(seeds[9], (D, GROUPS), D ** -0.5, 0.125),
        "expert_router": normal_values(seeds[10], (D, EXPERTS), D ** -0.5, 0.125),
        "routing": draw_routing(jax.random.fold_in(seeds[15], 71), 0),
        "expert_gate_w": normal_values(seeds[12], (EXPERTS, D, FF), D ** -0.5, 0.125, ((0, 16),)),
        "expert_up_w": normal_values(seeds[13], (EXPERTS, D, FF), D ** -0.5, 0.125, ((0, 16),)),
        "expert_down_w": normal_values(seeds[14], (EXPERTS, FF, D), FF ** -0.5, 0.25, ((0, 16),)),
    }


epsilon = 1e-06

def reference(conv_value, conv_gate, doc_ids, conv_kernel, norm_gain_conv, norm_bias_conv, proj_weight, residual, norm_gain_moe, group_router, expert_router, routing, expert_gate_w, expert_up_w, expert_down_w):
    gated_values = (conv_value.astype(jnp.float32) * jax.nn.sigmoid(conv_gate.astype(jnp.float32))).astype(jnp.bfloat16)
    rim_width = KW - 1
    length = gated_values.shape[0]
    padded = jnp.concatenate([jnp.zeros((rim_width, CH), jnp.bfloat16), gated_values], axis=0)
    padded_ids = jnp.concatenate([jnp.zeros((rim_width,), jnp.int32), doc_ids.astype(jnp.int32)], axis=0)
    kernel = conv_kernel.astype(jnp.float32)
    summed = jnp.zeros((length, CH), jnp.float32)
    for tap in range(KW):
        same_doc = padded_ids[tap:tap + length] == doc_ids
        summed = summed + jnp.where(same_doc[:, None], padded[tap:tap + length].astype(jnp.float32) * kernel[tap][None, :], jnp.float32(0.0))
    convolved = summed.astype(jnp.bfloat16)
    values = convolved.astype(jnp.float32)
    average = lax.optimization_barrier(jnp.mean(values, axis=1, keepdims=True))
    centered = values - average
    variance = lax.optimization_barrier(jnp.mean(centered * centered, axis=1, keepdims=True))
    activated = jax.nn.silu(centered * lax.rsqrt(variance + epsilon) * norm_gain_conv + norm_bias_conv).astype(jnp.bfloat16)
    projected = jnp.dot(activated, proj_weight, preferred_element_type=jnp.float32)
    hidden_state = (residual.astype(jnp.float32) + projected).astype(jnp.bfloat16)
    state_values = hidden_state.astype(jnp.float32)
    normed = (state_values * lax.rsqrt(lax.optimization_barrier(jnp.mean(state_values * state_values, axis=1, keepdims=True)) + epsilon) * norm_gain_moe).astype(jnp.bfloat16)
    group_logits = jnp.dot(normed, group_router, preferred_element_type=jnp.float32)
    expert_logits = jnp.dot(normed, expert_router, preferred_element_type=jnp.float32)
    per_group = EXPERTS // GROUPS
    chosen_group = (routing[:, 0] // per_group).astype(jnp.int32)
    group_exp = jnp.exp(group_logits)
    group_prob = jnp.take_along_axis(group_exp, chosen_group[:, None], axis=1)[:, 0] / lax.optimization_barrier(jnp.sum(group_exp, axis=1))
    first_logit = jnp.take_along_axis(expert_logits, routing[:, 0:1], axis=1)[:, 0]
    second_logit = jnp.take_along_axis(expert_logits, routing[:, 1:2], axis=1)[:, 0]
    first_exp = jnp.exp(first_logit)
    second_exp = jnp.exp(second_logit)
    first_weight = group_prob * first_exp / (first_exp + second_exp)
    second_weight = group_prob * second_exp / (first_exp + second_exp)
    per_expert = 2 * length // EXPERTS
    flat_experts = routing.reshape(-1).astype(jnp.int32)
    ordering = jnp.argsort(flat_experts, stable=True).astype(jnp.int32)
    slot_table = ordering.reshape(EXPERTS, per_expert)

    def one_expert(operands):
        assigned, gate_matrix, up_matrix, down_matrix = operands
        token_rows = normed[assigned // 2]
        gate_part = jnp.dot(token_rows, gate_matrix, preferred_element_type=jnp.float32)
        up_part = jnp.dot(token_rows, up_matrix, preferred_element_type=jnp.float32)
        expert_hidden = (jax.nn.silu(gate_part) * up_part).astype(jnp.bfloat16)
        return jnp.dot(expert_hidden, down_matrix, preferred_element_type=jnp.float32).astype(jnp.bfloat16)
    results = lax.map(one_expert, (slot_table, expert_gate_w, expert_up_w, expert_down_w))
    per_assignment = jnp.zeros((2 * length, D), jnp.bfloat16).at[slot_table.reshape(-1)].set(results.reshape(-1, D))
    picked = per_assignment.reshape(length, 2, D).astype(jnp.float32)
    mixture = first_weight[:, None] * picked[:, 0] + second_weight[:, None] * picked[:, 1]
    return (state_values + mixture).astype(jnp.bfloat16)
```

```python
import functools

import jax
import jax.numpy as jnp
from jax import lax
from jax.experimental import pallas as pl
from jax.experimental.pallas import tpu as pltpu
from jax.sharding import PartitionSpec as P

epsilon = 1e-06
TILE = 256
CHUNK = 64
VMEM = pl.BlockSpec(memory_space=pltpu.VMEM)
SMEM = pl.BlockSpec(memory_space=pltpu.SMEM)


def params(mib):
    return pltpu.CompilerParams(vmem_limit_bytes=mib * 1024 * 1024)


def conv_kernel_body(
    starts_ref, edge_ref, value_ref, gate_ref, rim_ref, kernel_ref, out_ref, taps, rows, masked, total
):
    step = pl.program_id(0)
    tile, lanes = value_ref.shape
    tap_count = kernel_ref.shape[0]

    @pl.when(step == 0)
    def _():
        kernel = kernel_ref[...].astype(jnp.float32)
        for tap in range(tap_count):
            taps[8 * tap : 8 * tap + 8, :] = jnp.broadcast_to(kernel[tap : tap + 1, :], (8, lanes))
        rows[0:32, :] = rim_ref[...].astype(jnp.float32)

    @pl.when(step > 0)
    def _():
        rows[0:32, :] = rows[tile : tile + 32, :]

    rows[32:, :] = (
        (value_ref[...].astype(jnp.float32) * jax.nn.sigmoid(gate_ref[...].astype(jnp.float32)))
        .astype(jnp.bfloat16)
        .astype(jnp.float32)
    )

    def convolve(source, at):
        acc = jnp.zeros((CHUNK // 8, 8, lanes), jnp.float32)
        for tap in range(tap_count):
            window = source[at + 2 + tap : at + 2 + tap + CHUNK, :].reshape(CHUNK // 8, 8, lanes)
            acc = acc + window * taps[8 * tap : 8 * tap + 8, :][None]
        return acc.reshape(CHUNK, lanes)

    low, high = edge_ref[0, step], edge_ref[1, step]
    whole = jnp.logical_and(low == high, starts_ref[low] <= step * tile)

    @pl.when(whole)
    def _():
        for at in range(0, tile, CHUNK):
            out_ref[at : at + CHUNK, :] = convolve(rows, at).astype(out_ref.dtype)

    @pl.when(jnp.logical_not(whole))
    def _():
        total[...] = jnp.zeros_like(total)

        def one_document(doc, carry):
            first = starts_ref[doc] - step * tile + 2
            last = starts_ref[doc + 1] - step * tile + 2
            position = lax.broadcasted_iota(jnp.int32, rows.shape, 0)
            masked[...] = jnp.where(
                jnp.logical_and(position >= first, position < last), rows[...], jnp.float32(0.0)
            )
            for at in range(0, tile, CHUNK):
                place = lax.broadcasted_iota(jnp.int32, (CHUNK, lanes), 0) + (at + 32)
                inside = jnp.logical_and(place >= first, place < last)
                total[at : at + CHUNK, :] += jnp.where(
                    inside, convolve(masked, at), jnp.float32(0.0)
                )
            return carry

        lax.fori_loop(low, high + 1, one_document, 0)
        out_ref[...] = total[...].astype(out_ref.dtype)


def convolve_tokens(starts, edges, value, gate, rim, kernel):
    tokens, lanes = value.shape
    taps = kernel.shape[0]
    return pl.pallas_call(
        conv_kernel_body,
        grid=(tokens // TILE,),
        in_specs=[
            SMEM,
            SMEM,
            pl.BlockSpec((TILE, lanes), lambda i: (i, 0)),
            pl.BlockSpec((TILE, lanes), lambda i: (i, 0)),
            pl.BlockSpec((32, lanes), lambda i: (0, 0)),
            pl.BlockSpec((taps, lanes), lambda i: (0, 0)),
        ],
        out_specs=pl.BlockSpec((TILE, lanes), lambda i: (i, 0)),
        out_shape=jax.ShapeDtypeStruct((tokens, lanes), jnp.bfloat16),
        scratch_shapes=[
            pltpu.VMEM((8 * taps, lanes), jnp.float32),
            pltpu.VMEM((TILE + 32, lanes), jnp.float32),
            pltpu.VMEM((TILE + 32, lanes), jnp.float32),
            pltpu.VMEM((TILE, lanes), jnp.float32),
        ],
        compiler_params=params(8),
        name="gated_conv",
    )(starts, edges, value, gate, rim, kernel)


def slots_body(capacity, routing_ref, routing_t_ref, spread_ref, first_ref, second_ref):
    count = routing_ref.shape[0]
    slots = spread_ref.shape[0]
    row = lax.broadcasted_iota(jnp.int32, (count, count), 0)
    column = lax.broadcasted_iota(jnp.int32, (count, count), 1)

    def ones(mask):
        return jnp.where(mask, jnp.float32(1.0), jnp.float32(0.0))

    lane = lax.broadcasted_iota(jnp.int32, (count, 128), 1)
    one, two = routing_ref[:, 0:1], routing_ref[:, 1:2]
    named = jnp.logical_or(lane == one, lane == two)
    before = jnp.dot(
        ones(column < row).astype(jnp.bfloat16),
        ones(named).astype(jnp.bfloat16),
        preferred_element_type=jnp.float32,
    )
    slot = lax.broadcasted_iota(jnp.int32, (count, slots), 1)
    for chosen, out in ((one, first_ref), (two, second_ref)):
        place = jnp.sum(jnp.where(lane == chosen, before, 0.0), axis=1, keepdims=True)
        target = chosen * capacity + place.astype(jnp.int32)
        out[...] = ones(slot == target).astype(jnp.bfloat16)

    sub = lax.broadcasted_iota(jnp.int32, (16, count), 0)
    one, two = routing_t_ref[0:1, :], routing_t_ref[1:2, :]
    named = jnp.logical_or(sub == one, sub == two)
    before = jnp.dot(
        ones(named).astype(jnp.bfloat16),
        ones(row < column).astype(jnp.bfloat16),
        preferred_element_type=jnp.float32,
    )
    slot = lax.broadcasted_iota(jnp.int32, (slots, count), 0)
    targets = []
    for chosen in (one, two):
        place = jnp.sum(jnp.where(sub == chosen, before, 0.0), axis=0, keepdims=True)
        targets.append(chosen * capacity + place.astype(jnp.int32))
    spread_ref[...] = ones(jnp.logical_or(slot == targets[0], slot == targets[1])).astype(
        jnp.bfloat16
    )


def project_body(
    groups,
    experts,
    raw_ref,
    weight_ref,
    gain_ref,
    bias_ref,
    residual_ref,
    gain_moe_ref,
    router_ref,
    routing_ref,
    spread_ref,
    state_ref,
    outgoing_ref,
    mix_ref,
    active,
    weight,
    sem,
):
    parts, count, lanes = raw_ref.shape
    width = parts * lanes
    pieces = weight.shape[0] // 512
    copies = []
    for piece in range(pieces):
        copy = pltpu.make_async_copy(
            weight_ref.at[512 * piece : 512 * piece + 512, :],
            weight.at[512 * piece : 512 * piece + 512, :],
            sem.at[piece],
        )
        copy.start()
        copies.append(copy)
    summed = jnp.zeros((count, lanes), jnp.float32)
    for part in range(parts):
        summed = summed + raw_ref[part].astype(jnp.float32)
    average = jnp.sum(summed, axis=1, keepdims=True) * jnp.float32(1.0 / width)
    squares = jnp.zeros((count, lanes), jnp.float32)
    for part in range(parts):
        centered = raw_ref[part].astype(jnp.float32) - average
        squares = squares + centered * centered
    variance = jnp.sum(squares, axis=1, keepdims=True) * jnp.float32(1.0 / width)
    scale = lax.rsqrt(variance + epsilon)
    for part in range(parts):
        at = slice(part * lanes, part * lanes + lanes)
        value = (raw_ref[part].astype(jnp.float32) - average) * scale * gain_ref[:, at] + bias_ref[
            :, at
        ]
        active[:, at] = jax.nn.silu(value).astype(jnp.bfloat16)
    projected = residual_ref[...].astype(jnp.float32)
    for piece in range(pieces):
        copies[piece].wait()
        at = slice(512 * piece, 512 * piece + 512)
        projected = projected + jnp.dot(
            active[:, at], weight[at, :], preferred_element_type=jnp.float32
        )
    state = projected.astype(jnp.bfloat16)
    state_ref[...] = state
    state = state.astype(jnp.float32)
    power = jnp.mean(state * state, axis=1, keepdims=True)
    normed = (state * lax.rsqrt(power + epsilon) * gain_moe_ref[...]).astype(jnp.bfloat16)
    outgoing_ref[...] = jnp.dot(
        spread_ref[...], normed, preferred_element_type=jnp.float32
    ).astype(jnp.bfloat16)
    logits = jnp.dot(normed, router_ref[...], preferred_element_type=jnp.float32)
    lane = lax.broadcasted_iota(jnp.int32, logits.shape, 1)
    one, two = routing_ref[:, 0:1], routing_ref[:, 1:2]
    group = one // (experts // groups)

    def pick(mask, array):
        return jnp.sum(jnp.where(mask, array, jnp.float32(0.0)), axis=1, keepdims=True)

    raised = jnp.exp(logits)
    in_groups = jnp.logical_and(lane >= experts, lane < experts + groups)
    group_prob = pick(lane == experts + group, raised) / pick(in_groups, raised)
    first = jnp.exp(pick(lane == one, logits))
    second = jnp.exp(pick(lane == two, logits))
    both = first + second
    mix_ref[...] = jnp.where(
        lane == 0, group_prob * first / both, jnp.where(lane == 1, group_prob * second / both, 0.0)
    )


def experts_body(rows_ref, gate_ref, up_ref, down_ref, out_ref):
    rows = rows_ref[...]
    gate = jnp.dot(rows, gate_ref[...], preferred_element_type=jnp.float32)
    up = jnp.dot(rows, up_ref[...], preferred_element_type=jnp.float32)
    hidden = (jax.nn.silu(gate) * up).astype(jnp.bfloat16)
    out_ref[...] = jnp.dot(hidden, down_ref[...], preferred_element_type=jnp.float32).astype(
        jnp.bfloat16
    )


def mix_body(state_ref, returned_ref, first_ref, second_ref, mix_ref, out_ref):
    returned = returned_ref[...]
    first = jnp.dot(first_ref[...], returned, preferred_element_type=jnp.float32)
    second = jnp.dot(second_ref[...], returned, preferred_element_type=jnp.float32)
    mixture = mix_ref[:, 0:1] * first + mix_ref[:, 1:2] * second
    out_ref[...] = (state_ref[...].astype(jnp.float32) + mixture).astype(jnp.bfloat16)


def shifted(array, axis, by):
    count = lax.axis_size(axis)
    pairs = [(i, i + by) for i in range(count) if 0 <= i + by < count]
    return lax.ppermute(array, axis, pairs)


def body(
    conv_value,
    conv_gate,
    doc_ids,
    conv_kernel,
    norm_gain_conv,
    norm_bias_conv,
    proj_weight,
    residual,
    norm_gain_moe,
    group_router,
    expert_router,
    routing,
    expert_gate_w,
    expert_up_w,
    expert_down_w,
):
    tokens, lanes = conv_value.shape
    rim = conv_kernel.shape[0] - 1
    count, width = residual.shape
    groups, experts = group_router.shape[1], expert_router.shape[1]
    slots = 2 * count
    capacity = slots // experts

    tail = slice(tokens - 32, tokens)
    tail_values = (
        conv_value[tail].astype(jnp.float32) * jax.nn.sigmoid(conv_gate[tail].astype(jnp.float32))
    ).astype(jnp.bfloat16)
    tail_ids = jnp.broadcast_to(doc_ids[tail][:, None], (32, lanes)).astype(jnp.bfloat16)
    came = shifted(jnp.concatenate([tail_values, tail_ids], axis=0), "sp", 1)
    rim_values, rim_ids = came[:32], came[64 - rim :, 0].astype(jnp.int32)
    padded_ids = jnp.concatenate([rim_ids, doc_ids], axis=0)
    bounds = jnp.arange(24, dtype=jnp.int32)
    starts = jnp.sum((padded_ids[None, :] < bounds[:, None]).astype(jnp.int32), axis=1)
    tiles = doc_ids.reshape(tokens // TILE, TILE)
    edges = jnp.stack([tiles[:, 0], tiles[:, -1]])
    convolved = convolve_tokens(starts, edges, conv_value, conv_gate, rim_values, conv_kernel)
    raw_rows = lax.all_to_all(
        convolved.reshape(-1, count, lanes), "tp", split_axis=0, concat_axis=0, tiled=True
    )

    spread, first_pick, second_pick = pl.pallas_call(
        functools.partial(slots_body, capacity),
        in_specs=[VMEM] * 2,
        out_specs=[VMEM] * 3,
        out_shape=[
            jax.ShapeDtypeStruct((slots, count), jnp.bfloat16),
            jax.ShapeDtypeStruct((count, slots), jnp.bfloat16),
            jax.ShapeDtypeStruct((count, slots), jnp.bfloat16),
        ],
        compiler_params=params(8),
        name="slots",
    )(routing, routing.T)
    routers = jnp.concatenate(
        [
            expert_router,
            group_router,
            jnp.zeros((width, 128 - experts - groups), jnp.bfloat16),
        ],
        axis=1,
    )
    full_weight = lax.all_gather(proj_weight, "tp", axis=0, tiled=True)
    state, outgoing, mix = pl.pallas_call(
        functools.partial(project_body, groups, experts),
        in_specs=[VMEM, pl.BlockSpec(memory_space=pltpu.HBM)] + [VMEM] * 7,
        out_specs=[VMEM] * 3,
        out_shape=[
            jax.ShapeDtypeStruct((count, width), jnp.bfloat16),
            jax.ShapeDtypeStruct((slots, width), jnp.bfloat16),
            jax.ShapeDtypeStruct((count, 128), jnp.float32),
        ],
        scratch_shapes=[
            pltpu.VMEM((count, full_weight.shape[0]), jnp.bfloat16),
            pltpu.VMEM(full_weight.shape, jnp.bfloat16),
            pltpu.SemaphoreType.DMA((full_weight.shape[0] // 512,)),
        ],
        compiler_params=params(28),
        name="project",
    )(
        raw_rows,
        full_weight,
        norm_gain_conv[None, :],
        norm_bias_conv[None, :],
        residual,
        norm_gain_moe[None, :],
        routers,
        routing,
        spread,
    )
    arrived = lax.all_to_all(
        outgoing.reshape(experts, capacity, width), "sp", split_axis=0, concat_axis=0, tiled=True
    )
    result = pl.pallas_call(
        experts_body,
        in_specs=[VMEM] * 4,
        out_specs=VMEM,
        out_shape=jax.ShapeDtypeStruct((slots, width), jnp.bfloat16),
        compiler_params=params(24),
        name="experts",
    )(arrived.reshape(slots, width), expert_gate_w[0], expert_up_w[0], expert_down_w[0])
    returned = lax.all_to_all(
        result.reshape(experts, capacity, width), "sp", split_axis=0, concat_axis=0, tiled=True
    )
    return pl.pallas_call(
        mix_body,
        in_specs=[VMEM] * 5,
        out_specs=VMEM,
        out_shape=jax.ShapeDtypeStruct((count, width), jnp.bfloat16),
        compiler_params=params(16),
        name="mix",
    )(state, returned.reshape(slots, width), first_pick, second_pick, mix)


def solution(mesh):
    placed = (
        P("sp", "tp"),
        P("sp", "tp"),
        P("sp"),
        P(None, "tp"),
        P(),
        P(),
        P("tp", None),
        P(("sp", "tp"), None),
        P(),
        P(),
        P(),
        P(("sp", "tp"), None),
        P("sp", None, None),
        P("sp", None, None),
        P("sp", None, None),
    )
    return jax.shard_map(
        body, mesh=mesh, in_specs=placed, out_specs=P(("sp", "tp"), None), check_vma=False
    )
```

```python
import functools

import jax
import jax.numpy as jnp
from jax import lax
from jax.experimental import pallas as pl
from jax.experimental.pallas import tpu as pltpu
from jax.sharding import PartitionSpec as P

epsilon = 1e-06
CHUNK = 64
ORDER = (0, 4, 2, 6, 1, 5, 3, 7)
NEAR = (0, 1, 3, 2)
VMEM = pl.BlockSpec(memory_space=pltpu.VMEM)
SMEM = pl.BlockSpec(memory_space=pltpu.SMEM)


def params(mib):
    return pltpu.CompilerParams(vmem_limit_bytes=mib * 1024 * 1024)


def conv_kernel_body(
    place_ref,
    starts_ref,
    edge_ref,
    value_ref,
    gate_ref,
    value_halo_ref,
    gate_halo_ref,
    rim_ref,
    kernel_ref,
    *refs,
):
    outs, (taps, rows, masked, total) = refs[:-4], refs[-4:]
    step = pl.program_id(0)
    at_tile = step ^ place_ref[0]
    tile, lanes = value_ref.shape
    tap_count = kernel_ref.shape[0]

    def gated(value, gate):
        return (
            (value[...].astype(jnp.float32) * jax.nn.sigmoid(gate[...].astype(jnp.float32)))
            .astype(jnp.bfloat16)
            .astype(jnp.float32)
        )

    @pl.when(step == 0)
    def _():
        kernel = kernel_ref[...].astype(jnp.float32)
        for tap in range(tap_count):
            taps[8 * tap : 8 * tap + 8, :] = jnp.broadcast_to(kernel[tap : tap + 1, :], (8, lanes))

    @pl.when(at_tile == 0)
    def _():
        rows[0:32, :] = rim_ref[...].astype(jnp.float32)

    @pl.when(at_tile > 0)
    def _():
        rows[0:32, :] = gated(value_halo_ref, gate_halo_ref)

    rows[32:, :] = gated(value_ref, gate_ref)

    def convolve(source, at):
        acc = jnp.zeros((CHUNK // 8, 8, lanes), jnp.float32)
        for tap in range(tap_count):
            window = source[at + 2 + tap : at + 2 + tap + CHUNK, :].reshape(CHUNK // 8, 8, lanes)
            acc = acc + window * taps[8 * tap : 8 * tap + 8, :][None]
        return acc.reshape(CHUNK, lanes)

    base = at_tile * tile
    low, high = edge_ref[0, at_tile], edge_ref[1, at_tile]
    whole = jnp.logical_and(low == high, starts_ref[low] <= base)

    @pl.when(whole)
    def _():
        for at in range(0, tile, CHUNK):
            total[at : at + CHUNK, :] = convolve(rows, at)

    @pl.when(jnp.logical_not(whole))
    def _():
        total[...] = jnp.zeros_like(total)

        def one_document(doc, carry):
            first = starts_ref[doc] - base + 2
            last = starts_ref[doc + 1] - base + 2
            position = lax.broadcasted_iota(jnp.int32, rows.shape, 0)
            masked[...] = jnp.where(
                jnp.logical_and(position >= first, position < last), rows[...], jnp.float32(0.0)
            )
            for at in range(0, tile, CHUNK):
                place = lax.broadcasted_iota(jnp.int32, (CHUNK, lanes), 0) + (at + 32)
                inside = jnp.logical_and(place >= first, place < last)
                total[at : at + CHUNK, :] += jnp.where(
                    inside, convolve(masked, at), jnp.float32(0.0)
                )
            return carry

        lax.fori_loop(low, high + 1, one_document, 0)

    for slot, out in enumerate(outs):

        @pl.when(step == slot)
        def _(out=out):
            out[...] = total[...].astype(out.dtype)


def convolve_tokens(place, starts, edges, value, gate, rim, kernel, parts):
    tokens, lanes = value.shape
    taps = kernel.shape[0]
    tile = tokens // parts

    def here(i, place, *_):
        return (i ^ place[0], 0)

    def halo(i, place, *_):
        return (jnp.maximum((i ^ place[0]) * (tile // 32) - 1, 0), 0)

    def whole(i, *_):
        return (0, 0)

    return pl.pallas_call(
        conv_kernel_body,
        grid_spec=pltpu.PrefetchScalarGridSpec(
            num_scalar_prefetch=3,
            grid=(parts,),
            in_specs=[
                pl.BlockSpec((tile, lanes), here),
                pl.BlockSpec((tile, lanes), here),
                pl.BlockSpec((32, lanes), halo),
                pl.BlockSpec((32, lanes), halo),
                pl.BlockSpec((32, lanes), whole),
                pl.BlockSpec((taps, lanes), whole),
            ],
            out_specs=[pl.BlockSpec((tile, lanes), whole)] * parts,
            scratch_shapes=[
                pltpu.VMEM((8 * taps, lanes), jnp.float32),
                pltpu.VMEM((tile + 32, lanes), jnp.float32),
                pltpu.VMEM((tile + 32, lanes), jnp.float32),
                pltpu.VMEM((tile, lanes), jnp.float32),
            ],
        ),
        out_shape=[jax.ShapeDtypeStruct((tile, lanes), jnp.bfloat16)] * parts,
        compiler_params=params(12),
        name="gated_conv",
    )(place, starts, edges, value, gate, value, gate, rim, kernel)


def slots_body(capacity, routing_ref, routing_t_ref, spread_ref, first_ref, second_ref):
    count = routing_ref.shape[0]
    slots = spread_ref.shape[0]
    row = lax.broadcasted_iota(jnp.int32, (count, count), 0)
    column = lax.broadcasted_iota(jnp.int32, (count, count), 1)

    def ones(mask):
        return jnp.where(mask, jnp.float32(1.0), jnp.float32(0.0))

    lane = lax.broadcasted_iota(jnp.int32, (count, 128), 1)
    one, two = routing_ref[:, 0:1], routing_ref[:, 1:2]
    named = jnp.logical_or(lane == one, lane == two)
    before = jnp.dot(
        ones(column < row).astype(jnp.bfloat16),
        ones(named).astype(jnp.bfloat16),
        preferred_element_type=jnp.float32,
    )
    slot = lax.broadcasted_iota(jnp.int32, (count, slots), 1)
    for chosen, out in ((one, first_ref), (two, second_ref)):
        place = jnp.sum(jnp.where(lane == chosen, before, 0.0), axis=1, keepdims=True)
        target = chosen * capacity + place.astype(jnp.int32)
        out[...] = ones(slot == target).astype(jnp.bfloat16)

    sub = lax.broadcasted_iota(jnp.int32, (16, count), 0)
    one, two = routing_t_ref[0:1, :], routing_t_ref[1:2, :]
    named = jnp.logical_or(sub == one, sub == two)
    before = jnp.dot(
        ones(named).astype(jnp.bfloat16),
        ones(row < column).astype(jnp.bfloat16),
        preferred_element_type=jnp.float32,
    )
    slot = lax.broadcasted_iota(jnp.int32, (slots, count), 0)
    targets = []
    for chosen in (one, two):
        place = jnp.sum(jnp.where(sub == chosen, before, 0.0), axis=0, keepdims=True)
        targets.append(chosen * capacity + place.astype(jnp.int32))
    spread_ref[...] = ones(jnp.logical_or(slot == targets[0], slot == targets[1])).astype(
        jnp.bfloat16
    )


def stats_body(*refs):
    raw_refs, out_ref = refs[:-1], refs[-1]
    count, lanes = raw_refs[0].shape
    summed = jnp.zeros((count, lanes), jnp.float32)
    for raw in raw_refs:
        summed = summed + raw[...].astype(jnp.float32)
    average = jnp.sum(summed, axis=1, keepdims=True) * jnp.float32(1.0 / (lanes * len(raw_refs)))
    squares = jnp.zeros((count, lanes), jnp.float32)
    for raw in raw_refs:
        centered = raw[...].astype(jnp.float32) - average
        squares = squares + centered * centered
    squares = jnp.sum(squares, axis=1, keepdims=True)
    lane = lax.broadcasted_iota(jnp.int32, (count, lanes), 1)
    out_ref[...] = jnp.where(lane == 0, average, squares)


def activate_body(order, place_ref, mine_ref, other_ref, gain_ref, bias_ref, *refs):
    raw_refs, out_ref = refs[:-1], refs[-1]
    lanes = raw_refs[0].shape[1]
    half = lanes * len(raw_refs)
    mine, other = mine_ref[:, 0:1], other_ref[:, 0:1]
    average = (mine + other) * jnp.float32(0.5)
    apart = mine - other
    spread = mine_ref[:, 1:2] + other_ref[:, 1:2] + apart * apart * jnp.float32(half / 2)
    scale = lax.rsqrt(spread * jnp.float32(0.5 / half) + epsilon)
    for slot, raw in enumerate(raw_refs):
        part = 2 * (place_ref[0] ^ order[slot]) + place_ref[1]
        value = (raw[...].astype(jnp.float32) - average) * scale * gain_ref[part] + bias_ref[part]
        out_ref[:, slot * lanes : slot * lanes + lanes] = jax.nn.silu(value).astype(jnp.bfloat16)


def partial_body(place_ref, active_ref, *refs):
    pieces, (mine_ref, other_ref, weight, product, sems) = refs[:-5], refs[-5:]
    slots, depth, width = weight.shape
    half = depth // 2
    core, y, x = place_ref[1], place_ref[2], place_ref[3]
    copies = []
    for number, piece in enumerate(pieces):
        far = NEAR[number % 4]
        top = number < 4
        for nth, near in enumerate(NEAR):
            column = ((y ^ far) * 4 + (x ^ near)) if top else ((y ^ near) * 4 + (x ^ far))
            copy = pltpu.make_async_copy(
                piece.at[nth],
                weight.at[
                    :,
                    pl.ds(0 if top else half, half),
                    pl.ds(pl.multiple_of(column * 128, 128), 128),
                ],
                sems.at[4 * number + nth],
            )
            copy.start()
            copies.append(copy)
    for copy in copies:
        copy.wait()
    product[...] = jnp.dot(
        active_ref[...],
        weight[...].reshape(slots * depth, width),
        preferred_element_type=jnp.float32,
    )
    count = mine_ref.shape[0]
    mine_ref[...] = product[pl.ds(pl.multiple_of(core * count, count), count), :]
    other_ref[...] = product[pl.ds(pl.multiple_of((1 - core) * count, count), count), :].astype(
        other_ref.dtype
    )


def state_body(
    groups,
    experts,
    mine_ref,
    other_ref,
    residual_ref,
    gain_moe_ref,
    router_ref,
    routing_ref,
    spread_ref,
    state_ref,
    outgoing_ref,
    mix_ref,
):
    projected = (
        residual_ref[...].astype(jnp.float32) + mine_ref[...] + other_ref[...].astype(jnp.float32)
    )
    state = projected.astype(jnp.bfloat16)
    state_ref[...] = state
    state = state.astype(jnp.float32)
    power = jnp.mean(state * state, axis=1, keepdims=True)
    normed = (state * lax.rsqrt(power + epsilon) * gain_moe_ref[...]).astype(jnp.bfloat16)
    outgoing_ref[...] = jnp.dot(
        spread_ref[...], normed, preferred_element_type=jnp.float32
    ).astype(jnp.bfloat16)
    logits = jnp.dot(normed, router_ref[...], preferred_element_type=jnp.float32)
    lane = lax.broadcasted_iota(jnp.int32, logits.shape, 1)
    one, two = routing_ref[:, 0:1], routing_ref[:, 1:2]
    group = one // (experts // groups)

    def pick(mask, array):
        return jnp.sum(jnp.where(mask, array, jnp.float32(0.0)), axis=1, keepdims=True)

    raised = jnp.exp(logits)
    in_groups = jnp.logical_and(lane >= experts, lane < experts + groups)
    group_prob = pick(lane == experts + group, raised) / pick(in_groups, raised)
    first = jnp.exp(pick(lane == one, logits))
    second = jnp.exp(pick(lane == two, logits))
    both = first + second
    mix_ref[...] = jnp.where(
        lane == 0, group_prob * first / both, jnp.where(lane == 1, group_prob * second / both, 0.0)
    )


def experts_body(rows_ref, gate_ref, up_ref, down_ref, out_ref):
    rows = rows_ref[...]
    gate = jnp.dot(rows, gate_ref[...], preferred_element_type=jnp.float32)
    up = jnp.dot(rows, up_ref[...], preferred_element_type=jnp.float32)
    hidden = (jax.nn.silu(gate) * up).astype(jnp.bfloat16)
    out_ref[...] = jnp.dot(hidden, down_ref[...], preferred_element_type=jnp.float32).astype(
        jnp.bfloat16
    )


def mix_body(state_ref, returned_ref, first_ref, second_ref, mix_ref, out_ref):
    returned = returned_ref[...]
    first = jnp.dot(first_ref[...], returned, preferred_element_type=jnp.float32)
    second = jnp.dot(second_ref[...], returned, preferred_element_type=jnp.float32)
    mixture = mix_ref[:, 0:1] * first + mix_ref[:, 1:2] * second
    out_ref[...] = (state_ref[...].astype(jnp.float32) + mixture).astype(jnp.bfloat16)


def swap(array, dy=0, dx=0, dz=0, dc=0):
    flip = (dy * 4 + dx) * 16 + dz * 2 + dc
    return lax.ppermute(array, ("sp", "tp"), [(i, i ^ flip) for i in range(256)])


def shifted(array, axis, by):
    count = lax.axis_size(axis)
    pairs = [(i, i + by) for i in range(count) if 0 <= i + by < count]
    return lax.ppermute(array, axis, pairs)


def body(
    conv_value,
    conv_gate,
    doc_ids,
    conv_kernel,
    norm_gain_conv,
    norm_bias_conv,
    proj_weight,
    residual,
    norm_gain_moe,
    group_router,
    expert_router,
    routing,
    expert_gate_w,
    expert_up_w,
    expert_down_w,
):
    tokens, lanes = conv_value.shape
    rim = conv_kernel.shape[0] - 1
    count, width = residual.shape
    groups, experts = group_router.shape[1], expert_router.shape[1]
    slots = 2 * count
    capacity = slots // experts

    sp, tp = lax.axis_index("sp"), lax.axis_index("tp")
    z, core, y, x = tp // 2, tp % 2, sp // 4, sp % 4
    place = jnp.stack([z, core, y, x]).astype(jnp.int32)
    depth = proj_weight.shape[0]

    tail = slice(tokens - 32, tokens)
    tail_values = (
        conv_value[tail].astype(jnp.float32) * jax.nn.sigmoid(conv_gate[tail].astype(jnp.float32))
    ).astype(jnp.bfloat16)
    tail_ids = jnp.broadcast_to(doc_ids[tail][:, None], (32, lanes)).astype(jnp.bfloat16)
    came = shifted(jnp.concatenate([tail_values, tail_ids], axis=0), "sp", 1)

    piece = lax.dynamic_slice_in_dim(proj_weight, sp * 128, 128, axis=1)
    held = jnp.stack([piece[: depth // 2], piece[depth // 2 :]])[:, None]
    for bit in (4, 2, 1):
        held = jnp.concatenate([held, swap(held, dz=bit)], axis=1)
    near_top = jnp.stack([held[0]] + [swap(held[0], dx=d) for d in (1, 3, 2)])
    near_low = jnp.stack([held[1]] + [swap(held[1], dy=d) for d in (1, 3, 2)])
    tops = [near_top] + [swap(near_top, dy=d) for d in (1, 3, 2)]
    lows = [near_low] + [swap(near_low, dx=d) for d in (1, 3, 2)]

    rim_values, rim_ids = came[:32], came[64 - rim :, 0].astype(jnp.int32)
    padded_ids = jnp.concatenate([rim_ids, doc_ids], axis=0)
    bounds = jnp.arange(24, dtype=jnp.int32)
    starts = jnp.sum((padded_ids[None, :] < bounds[:, None]).astype(jnp.int32), axis=1)
    tiles = doc_ids.reshape(8, tokens // 8)
    edges = jnp.stack([tiles[:, 0], tiles[:, -1]])
    convolved = convolve_tokens(
        place, starts, edges, conv_value, conv_gate, rim_values, conv_kernel, 8
    )
    raw = [convolved[d] if d == 0 else swap(convolved[d], dz=d) for d in ORDER]

    spread, first_pick, second_pick = pl.pallas_call(
        functools.partial(slots_body, capacity),
        in_specs=[VMEM] * 2,
        out_specs=[VMEM] * 3,
        out_shape=[
            jax.ShapeDtypeStruct((slots, count), jnp.bfloat16),
            jax.ShapeDtypeStruct((count, slots), jnp.bfloat16),
            jax.ShapeDtypeStruct((count, slots), jnp.bfloat16),
        ],
        compiler_params=params(8),
        name="slots",
    )(routing, routing.T)
    routers = jnp.concatenate(
        [
            expert_router,
            group_router,
            jnp.zeros((width, 128 - experts - groups), jnp.bfloat16),
        ],
        axis=1,
    )
    rows = 2 * count
    mine = pl.pallas_call(
        stats_body,
        in_specs=[VMEM] * 8,
        out_specs=VMEM,
        out_shape=jax.ShapeDtypeStruct((rows, lanes), jnp.float32),
        compiler_params=params(8),
        name="stats",
    )(*raw)
    other = swap(mine, dc=1)
    active = pl.pallas_call(
        functools.partial(activate_body, ORDER),
        in_specs=[SMEM] + [VMEM] * 12,
        out_specs=VMEM,
        out_shape=jax.ShapeDtypeStruct((rows, 8 * lanes), jnp.bfloat16),
        compiler_params=params(8),
        name="activate",
    )(
        place,
        mine,
        other,
        norm_gain_conv.reshape(-1, 1, lanes),
        norm_bias_conv.reshape(-1, 1, lanes),
        *raw,
    )
    kept, given = pl.pallas_call(
        partial_body,
        in_specs=[SMEM, VMEM] + [pl.BlockSpec(memory_space=pltpu.HBM)] * 8,
        out_specs=[VMEM] * 2,
        out_shape=[
            jax.ShapeDtypeStruct((count, width), jnp.float32),
            jax.ShapeDtypeStruct((count, width), jnp.bfloat16),
        ],
        scratch_shapes=[
            pltpu.VMEM((8, depth, width), jnp.bfloat16),
            pltpu.VMEM((rows, width), jnp.float32),
            pltpu.SemaphoreType.DMA((32,)),
        ],
        compiler_params=params(24),
        name="partial",
    )(place, active, *tops, *lows)
    state, outgoing, mix = pl.pallas_call(
        functools.partial(state_body, groups, experts),
        in_specs=[VMEM] * 7,
        out_specs=[VMEM] * 3,
        out_shape=[
            jax.ShapeDtypeStruct((count, width), jnp.bfloat16),
            jax.ShapeDtypeStruct((slots, width), jnp.bfloat16),
            jax.ShapeDtypeStruct((count, 128), jnp.float32),
        ],
        compiler_params=params(24),
        name="state",
    )(
        kept,
        swap(given, dc=1),
        residual,
        norm_gain_moe[None, :],
        routers,
        routing,
        spread,
    )
    arrived = lax.all_to_all(
        outgoing.reshape(experts, capacity, width), "sp", split_axis=0, concat_axis=0, tiled=True
    )
    result = pl.pallas_call(
        experts_body,
        in_specs=[VMEM] * 4,
        out_specs=VMEM,
        out_shape=jax.ShapeDtypeStruct((slots, width), jnp.bfloat16),
        compiler_params=params(24),
        name="experts",
    )(arrived.reshape(slots, width), expert_gate_w[0], expert_up_w[0], expert_down_w[0])
    returned = lax.all_to_all(
        result.reshape(experts, capacity, width), "sp", split_axis=0, concat_axis=0, tiled=True
    )
    return pl.pallas_call(
        mix_body,
        in_specs=[VMEM] * 5,
        out_specs=VMEM,
        out_shape=jax.ShapeDtypeStruct((count, width), jnp.bfloat16),
        compiler_params=params(16),
        name="mix",
    )(state, returned.reshape(slots, width), first_pick, second_pick, mix)


def solution(mesh):
    placed = (
        P("sp", "tp"),
        P("sp", "tp"),
        P("sp"),
        P(None, "tp"),
        P(),
        P(),
        P("tp", None),
        P(("sp", "tp"), None),
        P(),
        P(),
        P(),
        P(("sp", "tp"), None),
        P("sp", None, None),
        P("sp", None, None),
        P("sp", None, None),
    )
    return jax.shard_map(
        body, mesh=mesh, in_specs=placed, out_specs=P(("sp", "tp"), None), check_vma=False
    )
```

```python
import functools

import jax
import jax.numpy as jnp
from jax import lax
from jax.experimental import pallas as pl
from jax.experimental.pallas import tpu as pltpu
from jax.sharding import PartitionSpec as P

epsilon = 1e-06
CHUNK = 64
ORDER = (0, 4, 2, 6, 1, 5, 3, 7)
NEAR = (0, 1, 3, 2)
VMEM = pl.BlockSpec(memory_space=pltpu.VMEM)
SMEM = pl.BlockSpec(memory_space=pltpu.SMEM)


def params(mib):
    return pltpu.CompilerParams(vmem_limit_bytes=mib * 1024 * 1024)


def conv_kernel_body(
    place_ref,
    starts_ref,
    edge_ref,
    value_ref,
    gate_ref,
    value_halo_ref,
    gate_halo_ref,
    rim_ref,
    kernel_ref,
    *refs,
):
    outs, (taps, rows, masked, total) = refs[:-4], refs[-4:]
    step = pl.program_id(0)
    at_tile = step ^ place_ref[0]
    tile, lanes = value_ref.shape
    tap_count = kernel_ref.shape[0]

    def gated(value, gate):
        return (
            (value[...].astype(jnp.float32) * jax.nn.sigmoid(gate[...].astype(jnp.float32)))
            .astype(jnp.bfloat16)
            .astype(jnp.float32)
        )

    @pl.when(step == 0)
    def _():
        kernel = kernel_ref[...].astype(jnp.float32)
        for tap in range(tap_count):
            taps[8 * tap : 8 * tap + 8, :] = jnp.broadcast_to(kernel[tap : tap + 1, :], (8, lanes))

    @pl.when(at_tile == 0)
    def _():
        rows[0:32, :] = rim_ref[...].astype(jnp.float32)

    @pl.when(at_tile > 0)
    def _():
        rows[0:32, :] = gated(value_halo_ref, gate_halo_ref)

    rows[32:, :] = gated(value_ref, gate_ref)

    def convolve(source, at):
        acc = jnp.zeros((CHUNK // 8, 8, lanes), jnp.float32)
        for tap in range(tap_count):
            window = source[at + 2 + tap : at + 2 + tap + CHUNK, :].reshape(CHUNK // 8, 8, lanes)
            acc = acc + window * taps[8 * tap : 8 * tap + 8, :][None]
        return acc.reshape(CHUNK, lanes)

    base = at_tile * tile
    low, high = edge_ref[0, at_tile], edge_ref[1, at_tile]
    whole = jnp.logical_and(low == high, starts_ref[low] <= base)

    @pl.when(whole)
    def _():
        for at in range(0, tile, CHUNK):
            total[at : at + CHUNK, :] = convolve(rows, at)

    @pl.when(jnp.logical_not(whole))
    def _():
        total[...] = jnp.zeros_like(total)

        def one_document(doc, carry):
            first = starts_ref[doc] - base + 2
            last = starts_ref[doc + 1] - base + 2
            position = lax.broadcasted_iota(jnp.int32, rows.shape, 0)
            masked[...] = jnp.where(
                jnp.logical_and(position >= first, position < last), rows[...], jnp.float32(0.0)
            )
            for at in range(0, tile, CHUNK):
                place = lax.broadcasted_iota(jnp.int32, (CHUNK, lanes), 0) + (at + 32)
                inside = jnp.logical_and(place >= first, place < last)
                total[at : at + CHUNK, :] += jnp.where(
                    inside, convolve(masked, at), jnp.float32(0.0)
                )
            return carry

        lax.fori_loop(low, high + 1, one_document, 0)

    for slot, out in enumerate(outs):

        @pl.when(step == slot)
        def _(out=out):
            out[...] = total[...].astype(out.dtype)


def convolve_tokens(place, starts, edges, value, gate, rim, kernel, parts):
    tokens, lanes = value.shape
    taps = kernel.shape[0]
    tile = tokens // parts

    def here(i, place, *_):
        return (i ^ place[0], 0)

    def halo(i, place, *_):
        return (jnp.maximum((i ^ place[0]) * (tile // 32) - 1, 0), 0)

    def whole(i, *_):
        return (0, 0)

    return pl.pallas_call(
        conv_kernel_body,
        grid_spec=pltpu.PrefetchScalarGridSpec(
            num_scalar_prefetch=3,
            grid=(parts,),
            in_specs=[
                pl.BlockSpec((tile, lanes), here),
                pl.BlockSpec((tile, lanes), here),
                pl.BlockSpec((32, lanes), halo),
                pl.BlockSpec((32, lanes), halo),
                pl.BlockSpec((32, lanes), whole),
                pl.BlockSpec((taps, lanes), whole),
            ],
            out_specs=[pl.BlockSpec((tile, lanes), whole)] * parts,
            scratch_shapes=[
                pltpu.VMEM((8 * taps, lanes), jnp.float32),
                pltpu.VMEM((tile + 32, lanes), jnp.float32),
                pltpu.VMEM((tile + 32, lanes), jnp.float32),
                pltpu.VMEM((tile, lanes), jnp.float32),
            ],
        ),
        out_shape=[jax.ShapeDtypeStruct((tile, lanes), jnp.bfloat16)] * parts,
        compiler_params=params(12),
        name="gated_conv",
    )(place, starts, edges, value, gate, value, gate, rim, kernel)


def slots_body(capacity, place_ref, routing_ref, spread_ref, first_ref, second_ref, choice_ref):
    count = routing_ref.shape[1]
    slots = spread_ref.shape[0]
    row = lax.broadcasted_iota(jnp.int32, (count, count), 0)
    column = lax.broadcasted_iota(jnp.int32, (count, count), 1)
    core, device = place_ref[1], place_ref[4]

    def ones(mask):
        return jnp.where(mask, jnp.float32(1.0), jnp.float32(0.0))

    def slot_of(expert, position):
        apart = expert ^ device
        swapped = (apart & 3) * 4 + (apart >> 2)
        return jnp.where(core == 0, swapped, apart) * capacity + position.astype(jnp.int32)

    sub = lax.broadcasted_iota(jnp.int32, (16, count), 0)
    one, two = routing_ref[0:1, :], routing_ref[1:2, :]
    named = jnp.logical_or(sub == one, sub == two)
    before = jnp.dot(
        ones(named).astype(jnp.bfloat16),
        ones(row < column).astype(jnp.bfloat16),
        preferred_element_type=jnp.float32,
    )
    slot = lax.broadcasted_iota(jnp.int32, (slots, count), 0)
    targets = []
    for chosen in (one, two):
        position = jnp.sum(jnp.where(sub == chosen, before, 0.0), axis=0, keepdims=True)
        targets.append(slot_of(chosen, position))
    spread_ref[...] = ones(jnp.logical_or(slot == targets[0], slot == targets[1])).astype(
        jnp.bfloat16
    )

    def upright(line):
        turned = jnp.sum(
            jnp.where(row == column, line.astype(jnp.float32), 0.0), axis=1, keepdims=True
        )
        return turned.astype(jnp.int32)

    slot = lax.broadcasted_iota(jnp.int32, (count, slots), 1)
    for target, out in zip(targets, (first_ref, second_ref), strict=True):
        out[...] = ones(slot == upright(target)).astype(jnp.bfloat16)
    lane = lax.broadcasted_iota(jnp.int32, choice_ref.shape, 1)
    choice_ref[...] = jnp.where(lane == 0, upright(one), upright(two))


def stats_body(*refs):
    raw_refs, out_ref = refs[:-1], refs[-1]
    count, lanes = raw_refs[0].shape
    summed = jnp.zeros((count, lanes), jnp.float32)
    for raw in raw_refs:
        summed = summed + raw[...].astype(jnp.float32)
    average = jnp.sum(summed, axis=1, keepdims=True) * jnp.float32(1.0 / (lanes * len(raw_refs)))
    squares = jnp.zeros((count, lanes), jnp.float32)
    for raw in raw_refs:
        centered = raw[...].astype(jnp.float32) - average
        squares = squares + centered * centered
    squares = jnp.sum(squares, axis=1, keepdims=True)
    lane = lax.broadcasted_iota(jnp.int32, (count, lanes), 1)
    out_ref[...] = jnp.where(lane == 0, average, squares)


def activate_body(order, place_ref, mine_ref, other_ref, gain_ref, bias_ref, *refs):
    raw_refs, out_ref = refs[:-1], refs[-1]
    rows, lanes = raw_refs[0].shape
    count = rows // 2
    half = lanes * len(raw_refs)
    core = place_ref[1]
    for block in range(2):
        at = pl.ds(pl.multiple_of((core ^ block) * count, count), count)
        to = slice(block * count, block * count + count)
        mine, other = mine_ref[at, :], other_ref[at, :]
        average = (mine[:, 0:1] + other[:, 0:1]) * jnp.float32(0.5)
        apart = mine[:, 0:1] - other[:, 0:1]
        spread = mine[:, 1:2] + other[:, 1:2] + apart * apart * jnp.float32(half / 2)
        scale = lax.rsqrt(spread * jnp.float32(0.5 / half) + epsilon)
        for slot, raw in enumerate(raw_refs):
            part = 2 * (place_ref[0] ^ order[slot]) + core
            value = (raw[at, :].astype(jnp.float32) - average) * scale * gain_ref[part] + bias_ref[
                part
            ]
            out_ref[to, slot * lanes : slot * lanes + lanes] = jax.nn.silu(value).astype(
                jnp.bfloat16
            )


def partial_body(place_ref, active_ref, *refs):
    pieces, (mine_ref, other_ref, weight, sems) = refs[:-4], refs[-4:]
    _, slots, depth, group = weight.shape
    count = mine_ref.shape[0]
    v, u = place_ref[2], place_ref[3]
    copies = []
    for number, piece in enumerate(pieces):
        for nth, near in enumerate(NEAR):
            copy = pltpu.make_async_copy(
                piece.at[nth],
                weight.at[number, :, :, pl.ds(pl.multiple_of((u ^ near) * 128, 128), 128)],
                sems.at[4 * number + nth],
            )
            copy.start()
            copies.append(copy)
    for number, far in enumerate(NEAR):
        for nth in range(4):
            copies[4 * number + nth].wait()
        product = jnp.dot(
            active_ref[...],
            weight[number].reshape(slots * depth, group),
            preferred_element_type=jnp.float32,
        )
        to = pl.ds(pl.multiple_of((v ^ far) * group, group), group)
        mine_ref[:, to] = product[:count]
        other_ref[:, to] = product[count:].astype(other_ref.dtype)


def state_body(
    groups,
    experts,
    mine_ref,
    other_ref,
    residual_ref,
    gain_moe_ref,
    router_ref,
    choice_ref,
    spread_ref,
    state_ref,
    mix_ref,
    *outgoing_refs,
):
    projected = (
        residual_ref[...].astype(jnp.float32) + mine_ref[...] + other_ref[...].astype(jnp.float32)
    )
    state = projected.astype(jnp.bfloat16)
    state_ref[...] = state
    state = state.astype(jnp.float32)
    power = jnp.mean(state * state, axis=1, keepdims=True)
    normed = (state * lax.rsqrt(power + epsilon) * gain_moe_ref[...]).astype(jnp.bfloat16)
    outgoing = jnp.dot(spread_ref[...], normed, preferred_element_type=jnp.float32)
    block = outgoing_refs[0].shape[0]
    for number, ref in enumerate(outgoing_refs):
        ref[...] = outgoing[number * block : number * block + block].astype(jnp.bfloat16)
    logits = lax.dot_general(
        normed, router_ref[...], (((1,), (1,)), ((), ())), preferred_element_type=jnp.float32
    )
    lane = lax.broadcasted_iota(jnp.int32, logits.shape, 1)
    one, two = choice_ref[:, 0:1], choice_ref[:, 1:2]
    group = one // (experts // groups)

    def pick(mask, array):
        return jnp.sum(jnp.where(mask, array, jnp.float32(0.0)), axis=1, keepdims=True)

    raised = jnp.exp(logits)
    in_groups = jnp.logical_and(lane >= experts, lane < experts + groups)
    group_prob = pick(lane == experts + group, raised) / pick(in_groups, raised)
    first = jnp.exp(pick(lane == one, logits))
    second = jnp.exp(pick(lane == two, logits))
    both = first + second
    mix_ref[...] = jnp.where(
        lane == 0, group_prob * first / both, jnp.where(lane == 1, group_prob * second / both, 0.0)
    )


def experts_body(rows_ref, gate_ref, up_ref, down_ref, out_ref):
    rows = rows_ref[...]
    gate = jnp.dot(rows, gate_ref[...], preferred_element_type=jnp.float32)
    up = jnp.dot(rows, up_ref[...], preferred_element_type=jnp.float32)
    hidden = (jax.nn.silu(gate) * up).astype(jnp.bfloat16)
    out_ref[...] = jnp.dot(hidden, down_ref[...], preferred_element_type=jnp.float32).astype(
        jnp.bfloat16
    )


def mix_body(state_ref, first_ref, second_ref, mix_ref, *refs):
    returned_refs, out_ref = refs[:-1], refs[-1]
    returned = jnp.concatenate([returned[...] for returned in returned_refs], axis=0)
    first = jnp.dot(first_ref[...], returned, preferred_element_type=jnp.float32)
    second = jnp.dot(second_ref[...], returned, preferred_element_type=jnp.float32)
    mixture = mix_ref[:, 0:1] * first + mix_ref[:, 1:2] * second
    out_ref[...] = (state_ref[...].astype(jnp.float32) + mixture).astype(jnp.bfloat16)


def swap(array, dz=0, dc=0):
    flip = dz * 2 + dc
    return lax.ppermute(array, ("sp", "tp"), [(i, i ^ flip) for i in range(256)])


def cross(array, by, turn):
    pairs = [(i, i ^ (by * (16 if (i & 1) == turn else 64))) for i in range(256)]
    return lax.ppermute(array, ("sp", "tp"), pairs)


def shifted(array, axis, by):
    count = lax.axis_size(axis)
    pairs = [(i, i + by) for i in range(count) if 0 <= i + by < count]
    return lax.ppermute(array, axis, pairs)


def body(
    conv_value,
    conv_gate,
    doc_ids,
    conv_kernel,
    norm_gain_conv,
    norm_bias_conv,
    proj_weight,
    residual,
    norm_gain_moe,
    group_router,
    expert_router,
    routing,
    expert_gate_w,
    expert_up_w,
    expert_down_w,
):
    tokens, lanes = conv_value.shape
    rim = conv_kernel.shape[0] - 1
    count, width = residual.shape
    groups, experts = group_router.shape[1], expert_router.shape[1]
    slots = 2 * count
    capacity = slots // experts

    sp, tp = lax.axis_index("sp"), lax.axis_index("tp")
    z, core, y, x = tp >> 1, tp & 1, sp >> 2, sp & 3
    u, v = jnp.where(core == 0, x, y), jnp.where(core == 0, y, x)
    place = jnp.stack([z, core, v, u, sp]).astype(jnp.int32)
    depth = proj_weight.shape[0]

    tail = slice(tokens - 32, tokens)
    tail_values = (
        conv_value[tail].astype(jnp.float32) * jax.nn.sigmoid(conv_gate[tail].astype(jnp.float32))
    ).astype(jnp.bfloat16)
    tail_ids = jnp.broadcast_to(doc_ids[tail][:, None], (32, lanes)).astype(jnp.bfloat16)
    came = shifted(jnp.concatenate([tail_values, tail_ids], axis=0), "sp", 1)

    held = lax.dynamic_slice_in_dim(proj_weight, (v * 4 + u) * 128, 128, axis=1)[None]
    for bit in (4, 2, 1):
        held = jnp.concatenate([held, swap(held, dz=bit)], axis=0)

    rim_values, rim_ids = came[:32], came[64 - rim :, 0].astype(jnp.int32)
    padded_ids = jnp.concatenate([rim_ids, doc_ids], axis=0)
    bounds = jnp.arange(24, dtype=jnp.int32)
    starts = jnp.sum((padded_ids[None, :] < bounds[:, None]).astype(jnp.int32), axis=1)
    tiles = doc_ids.reshape(8, tokens // 8)
    edges = jnp.stack([tiles[:, 0], tiles[:, -1]])
    convolved = convolve_tokens(
        place, starts, edges, conv_value, conv_gate, rim_values, conv_kernel, 8
    )
    held, convolved = lax.optimization_barrier((held, convolved))
    near = jnp.stack([held] + [cross(held, d, 0) for d in NEAR[1:]])
    pieces = [near] + [cross(near, d, 1) for d in NEAR[1:]]
    raw = [convolved[d] if d == 0 else swap(convolved[d], dz=d) for d in ORDER]

    spread, first_pick, second_pick, choice = pl.pallas_call(
        functools.partial(slots_body, capacity),
        in_specs=[SMEM, VMEM],
        out_specs=[VMEM] * 4,
        out_shape=[
            jax.ShapeDtypeStruct((slots, count), jnp.bfloat16),
            jax.ShapeDtypeStruct((count, slots), jnp.bfloat16),
            jax.ShapeDtypeStruct((count, slots), jnp.bfloat16),
            jax.ShapeDtypeStruct((count, 128), jnp.int32),
        ],
        compiler_params=params(8),
        name="slots",
    )(place, routing.T)
    routers = jnp.concatenate(
        [
            expert_router.T,
            group_router.T,
            jnp.zeros((32 - experts - groups, width), jnp.bfloat16),
        ],
        axis=0,
    )
    rows = 2 * count
    mine = pl.pallas_call(
        stats_body,
        in_specs=[VMEM] * 8,
        out_specs=VMEM,
        out_shape=jax.ShapeDtypeStruct((rows, lanes), jnp.float32),
        compiler_params=params(8),
        name="stats",
    )(*raw)
    other = swap(mine, dc=1)
    active = pl.pallas_call(
        functools.partial(activate_body, ORDER),
        in_specs=[SMEM] + [VMEM] * 12,
        out_specs=VMEM,
        out_shape=jax.ShapeDtypeStruct((rows, 8 * lanes), jnp.bfloat16),
        compiler_params=params(8),
        name="activate",
    )(
        place,
        mine,
        other,
        norm_gain_conv.reshape(-1, 1, lanes),
        norm_bias_conv.reshape(-1, 1, lanes),
        *raw,
    )
    kept, given = pl.pallas_call(
        partial_body,
        in_specs=[SMEM, VMEM] + [pl.BlockSpec(memory_space=pltpu.HBM)] * 4,
        out_specs=[VMEM] * 2,
        out_shape=[
            jax.ShapeDtypeStruct((count, width), jnp.float32),
            jax.ShapeDtypeStruct((count, width), jnp.bfloat16),
        ],
        scratch_shapes=[
            pltpu.VMEM((4, 8, depth, width // 4), jnp.bfloat16),
            pltpu.SemaphoreType.DMA((16,)),
        ],
        compiler_params=params(24),
        name="partial",
    )(place, active, *pieces)
    block = slots // 4
    state, mix, *outgoing = pl.pallas_call(
        functools.partial(state_body, groups, experts),
        in_specs=[VMEM] * 7,
        out_specs=[VMEM] * 6,
        out_shape=[
            jax.ShapeDtypeStruct((count, width), jnp.bfloat16),
            jax.ShapeDtypeStruct((count, 32), jnp.float32),
        ]
        + [jax.ShapeDtypeStruct((block, width), jnp.bfloat16)] * 4,
        compiler_params=params(24),
        name="state",
    )(
        kept,
        swap(given, dc=1),
        residual,
        norm_gain_moe[None, :],
        routers,
        choice,
        spread,
    )

    def regrouped(blocks, which):
        return jnp.concatenate(
            [blocks[i][which * capacity : which * capacity + capacity] for i in range(4)], axis=0
        )

    passing = {0: outgoing[0]} | {d: cross(outgoing[d], d, 0) for d in NEAR[1:]}
    arrived = {d: regrouped(passing, d) for d in NEAR}
    arrived = {d: cross(arrived[d], d, 1) if d else arrived[d] for d in NEAR}
    results = {
        d: pl.pallas_call(
            experts_body,
            in_specs=[VMEM] * 4,
            out_specs=VMEM,
            out_shape=jax.ShapeDtypeStruct((block, width), jnp.bfloat16),
            compiler_params=params(16),
            name="experts",
        )(arrived[d], expert_gate_w[0], expert_up_w[0], expert_down_w[0])
        for d in NEAR
    }
    results = {d: cross(results[d], d, 1) if d else results[d] for d in NEAR}
    returned = {d: regrouped(results, d) for d in NEAR}
    returned = {d: cross(returned[d], d, 0) if d else returned[d] for d in NEAR}
    return pl.pallas_call(
        mix_body,
        in_specs=[VMEM] * 8,
        out_specs=VMEM,
        out_shape=jax.ShapeDtypeStruct((count, width), jnp.bfloat16),
        compiler_params=params(16),
        name="mix",
    )(state, first_pick, second_pick, mix, *[returned[d] for d in range(4)])


def solution(mesh):
    placed = (
        P("sp", "tp"),
        P("sp", "tp"),
        P("sp"),
        P(None, "tp"),
        P(),
        P(),
        P("tp", None),
        P(("sp", "tp"), None),
        P(),
        P(),
        P(),
        P(("sp", "tp"), None),
        P("sp", None, None),
        P("sp", None, None),
        P("sp", None, None),
    )
    return jax.shard_map(
        body, mesh=mesh, in_specs=placed, out_specs=P(("sp", "tp"), None), check_vma=False
    )
```

```python
import functools

import jax
import jax.numpy as jnp
from jax import lax
from jax.experimental import pallas as pl
from jax.experimental.pallas import tpu as pltpu
from jax.sharding import PartitionSpec as P


epsilon = 1e-06
CHUNK = 64
ORDER = (0, 4, 2, 6, 1, 5, 3, 7)
NEAR = (0, 1, 3, 2)
VMEM = pl.BlockSpec(memory_space=pltpu.VMEM)
SMEM = pl.BlockSpec(memory_space=pltpu.SMEM)


def params(mib):
    return pltpu.CompilerParams(vmem_limit_bytes=mib * 1024 * 1024)


def conv_kernel_body(
    place_ref,
    starts_ref,
    edge_ref,
    value_ref,
    gate_ref,
    value_halo_ref,
    gate_halo_ref,
    rim_ref,
    kernel_ref,
    *refs,
):
    outs, (taps, rows, masked, total) = refs[:-4], refs[-4:]
    step = pl.program_id(0)
    at_tile = step ^ place_ref[0]
    tile, lanes = value_ref.shape
    tap_count = kernel_ref.shape[0]

    def gated(value, gate):
        return (
            (value[...].astype(jnp.float32) * jax.nn.sigmoid(gate[...].astype(jnp.float32)))
            .astype(jnp.bfloat16)
            .astype(jnp.float32)
        )

    @pl.when(step == 0)
    def _():
        kernel = kernel_ref[...].astype(jnp.float32)
        for tap in range(tap_count):
            taps[8 * tap : 8 * tap + 8, :] = jnp.broadcast_to(kernel[tap : tap + 1, :], (8, lanes))

    @pl.when(at_tile == 0)
    def _():
        rows[0:32, :] = rim_ref[...].astype(jnp.float32)

    @pl.when(at_tile > 0)
    def _():
        rows[0:32, :] = gated(value_halo_ref, gate_halo_ref)

    rows[32:, :] = gated(value_ref, gate_ref)

    def convolve(source, at):
        acc = jnp.zeros((CHUNK // 8, 8, lanes), jnp.float32)
        for tap in range(tap_count):
            window = source[at + 2 + tap : at + 2 + tap + CHUNK, :].reshape(CHUNK // 8, 8, lanes)
            acc = acc + window * taps[8 * tap : 8 * tap + 8, :][None]
        return acc.reshape(CHUNK, lanes)

    base = at_tile * tile
    low, high = edge_ref[0, at_tile], edge_ref[1, at_tile]
    whole = jnp.logical_and(low == high, starts_ref[low] <= base)

    @pl.when(whole)
    def _():
        for at in range(0, tile, CHUNK):
            total[at : at + CHUNK, :] = convolve(rows, at)

    @pl.when(jnp.logical_not(whole))
    def _():
        total[...] = jnp.zeros_like(total)

        def one_document(doc, carry):
            first = starts_ref[doc] - base + 2
            last = starts_ref[doc + 1] - base + 2
            position = lax.broadcasted_iota(jnp.int32, rows.shape, 0)
            masked[...] = jnp.where(
                jnp.logical_and(position >= first, position < last), rows[...], jnp.float32(0.0)
            )
            for at in range(0, tile, CHUNK):
                place = lax.broadcasted_iota(jnp.int32, (CHUNK, lanes), 0) + (at + 32)
                inside = jnp.logical_and(place >= first, place < last)
                total[at : at + CHUNK, :] += jnp.where(
                    inside, convolve(masked, at), jnp.float32(0.0)
                )
            return carry

        lax.fori_loop(low, high + 1, one_document, 0)

    for slot, out in enumerate(outs):

        @pl.when(step == slot)
        def _(out=out):
            out[...] = total[...].astype(out.dtype)


def convolve_tokens(place, starts, edges, value, gate, rim, kernel, parts):
    tokens, lanes = value.shape
    taps = kernel.shape[0]
    tile = tokens // parts

    def here(i, place, *_):
        return (i ^ place[0], 0)

    def halo(i, place, *_):
        return (jnp.maximum((i ^ place[0]) * (tile // 32) - 1, 0), 0)

    def whole(i, *_):
        return (0, 0)

    return pl.pallas_call(
        conv_kernel_body,
        grid_spec=pltpu.PrefetchScalarGridSpec(
            num_scalar_prefetch=3,
            grid=(parts,),
            in_specs=[
                pl.BlockSpec((tile, lanes), here),
                pl.BlockSpec((tile, lanes), here),
                pl.BlockSpec((32, lanes), halo),
                pl.BlockSpec((32, lanes), halo),
                pl.BlockSpec((32, lanes), whole),
                pl.BlockSpec((taps, lanes), whole),
            ],
            out_specs=[pl.BlockSpec((tile, lanes), whole)] * parts,
            scratch_shapes=[
                pltpu.VMEM((8 * taps, lanes), jnp.float32),
                pltpu.VMEM((tile + 32, lanes), jnp.float32),
                pltpu.VMEM((tile + 32, lanes), jnp.float32),
                pltpu.VMEM((tile, lanes), jnp.float32),
            ],
        ),
        out_shape=[jax.ShapeDtypeStruct((tile, lanes), jnp.bfloat16)] * parts,
        compiler_params=params(12),
        name="gated_conv",
    )(place, starts, edges, value, gate, value, gate, rim, kernel)


def rim_body(value_ref, gate_ref, ids_ref, out_ref):
    tokens, lanes = value_ref.shape
    tail = slice(tokens - 32, tokens)
    out_ref[0:32, :] = (
        value_ref[tail, :].astype(jnp.float32)
        * jax.nn.sigmoid(gate_ref[tail, :].astype(jnp.float32))
    ).astype(jnp.bfloat16)
    row = lax.broadcasted_iota(jnp.int32, (32, lanes), 0)
    ids = jnp.zeros((32, lanes), jnp.int32)
    for place in range(32):
        ids = jnp.where(row == place, ids_ref[tokens - 32 + place], ids)
    out_ref[32:64, :] = ids.astype(jnp.float32).astype(jnp.bfloat16)


def slots_body(capacity, place_ref, routing_ref, spread_ref, first_ref, second_ref, choice_ref):
    count = routing_ref.shape[1]
    slots = spread_ref.shape[0]
    row = lax.broadcasted_iota(jnp.int32, (count, count), 0)
    column = lax.broadcasted_iota(jnp.int32, (count, count), 1)
    role, device = place_ref[5], place_ref[4]

    def ones(mask):
        return jnp.where(mask, jnp.float32(1.0), jnp.float32(0.0))

    def slot_of(expert, position):
        apart = expert ^ device
        swapped = (apart & 3) * 4 + (apart >> 2)
        return jnp.where(role == 0, swapped, apart) * capacity + position.astype(jnp.int32)

    sub = lax.broadcasted_iota(jnp.int32, (16, count), 0)
    one, two = routing_ref[0:1, :], routing_ref[1:2, :]
    named = jnp.logical_or(sub == one, sub == two)
    before = jnp.dot(
        ones(named).astype(jnp.bfloat16),
        ones(row < column).astype(jnp.bfloat16),
        preferred_element_type=jnp.float32,
    )
    slot = lax.broadcasted_iota(jnp.int32, (slots, count), 0)
    targets = []
    for chosen in (one, two):
        position = jnp.sum(jnp.where(sub == chosen, before, 0.0), axis=0, keepdims=True)
        targets.append(slot_of(chosen, position))
    spread_ref[...] = ones(jnp.logical_or(slot == targets[0], slot == targets[1])).astype(
        jnp.bfloat16
    )

    def upright(line):
        turned = jnp.sum(
            jnp.where(row == column, line.astype(jnp.float32), 0.0), axis=1, keepdims=True
        )
        return turned.astype(jnp.int32)

    slot = lax.broadcasted_iota(jnp.int32, (count, slots), 1)
    for target, out in zip(targets, (first_ref, second_ref), strict=True):
        out[...] = ones(slot == upright(target)).astype(jnp.bfloat16)
    lane = lax.broadcasted_iota(jnp.int32, choice_ref.shape, 1)
    choice_ref[...] = jnp.where(lane == 0, upright(one), upright(two))


def stats_body(*refs):
    raw_refs, out_ref = refs[:-1], refs[-1]
    count, lanes = raw_refs[0].shape
    summed = jnp.zeros((count, lanes), jnp.float32)
    for raw in raw_refs:
        summed = summed + raw[...].astype(jnp.float32)
    average = jnp.sum(summed, axis=1, keepdims=True) * jnp.float32(1.0 / (lanes * len(raw_refs)))
    squares = jnp.zeros((count, lanes), jnp.float32)
    for raw in raw_refs:
        centered = raw[...].astype(jnp.float32) - average
        squares = squares + centered * centered
    squares = jnp.sum(squares, axis=1, keepdims=True)
    lane = lax.broadcasted_iota(jnp.int32, (count, lanes), 1)
    out_ref[...] = jnp.where(lane == 0, average, squares)


def activate_body(order, place_ref, mine_ref, other_ref, gain_ref, bias_ref, *refs):
    raw_refs, out_ref = refs[:-1], refs[-1]
    rows, lanes = raw_refs[0].shape
    count = rows // 2
    half = lanes * len(raw_refs)
    core = place_ref[1]
    for block in range(2):
        at = pl.ds(pl.multiple_of((core ^ block) * count, count), count)
        to = slice(block * count, block * count + count)
        mine, other = mine_ref[at, :], other_ref[at, :]
        average = (mine[:, 0:1] + other[:, 0:1]) * jnp.float32(0.5)
        apart = mine[:, 0:1] - other[:, 0:1]
        spread = mine[:, 1:2] + other[:, 1:2] + apart * apart * jnp.float32(half / 2)
        scale = lax.rsqrt(spread * jnp.float32(0.5 / half) + epsilon)
        for slot, raw in enumerate(raw_refs):
            part = 2 * (place_ref[0] ^ order[slot]) + core
            value = (raw[at, :].astype(jnp.float32) - average) * scale * gain_ref[part] + bias_ref[
                part
            ]
            out_ref[to, slot * lanes : slot * lanes + lanes] = jax.nn.silu(value).astype(
                jnp.bfloat16
            )


def partial_body(
    place_ref,
    active_ref,
    low_ref,
    low_1_ref,
    low_32_ref,
    high_ref,
    high_3_ref,
    high_12_ref,
    mine_ref,
    other_ref,
    weight,
    sems,
):
    _, slots, depth, group = weight.shape
    count = mine_ref.shape[0]
    v, u = place_ref[2], place_ref[3]
    sources = (
        (0, low_ref, high_ref),
        (1, low_1_ref, high_12_ref.at[0]),
        (3, low_32_ref.at[0], high_3_ref),
        (2, low_32_ref.at[1], high_12_ref.at[1]),
    )
    copies = []
    for number, (_, *halves) in enumerate(sources):
        for side, half in enumerate(halves):
            for nth, near in enumerate(NEAR):
                copy = pltpu.make_async_copy(
                    half.at[nth],
                    weight.at[
                        number,
                        pl.ds(4 * side, 4),
                        :,
                        pl.ds(pl.multiple_of((u ^ near) * 128, 128), 128),
                    ],
                    sems.at[8 * number + 4 * side + nth],
                )
                copy.start()
                copies.append(copy)
    for number, (far, *_) in enumerate(sources):
        for nth in range(8):
            copies[8 * number + nth].wait()
        product = jnp.dot(
            active_ref[...],
            weight[number].reshape(slots * depth, group),
            preferred_element_type=jnp.float32,
        )
        to = pl.ds(pl.multiple_of((v ^ far) * group, group), group)
        mine_ref[:, to] = product[:count]
        other_ref[:, to] = product[count:].astype(other_ref.dtype)


def state_body(
    groups,
    experts,
    mine_ref,
    other_ref,
    residual_ref,
    gain_moe_ref,
    router_ref,
    choice_ref,
    spread_ref,
    state_ref,
    mix_ref,
    *outgoing_refs,
):
    projected = (
        residual_ref[...].astype(jnp.float32) + mine_ref[...] + other_ref[...].astype(jnp.float32)
    )
    state = projected.astype(jnp.bfloat16)
    state_ref[...] = state
    state = state.astype(jnp.float32)
    power = jnp.mean(state * state, axis=1, keepdims=True)
    normed = (state * lax.rsqrt(power + epsilon) * gain_moe_ref[...]).astype(jnp.bfloat16)
    outgoing = jnp.dot(spread_ref[...], normed, preferred_element_type=jnp.float32)
    block = outgoing_refs[0].shape[0]
    for number, ref in enumerate(outgoing_refs):
        ref[...] = outgoing[number * block : number * block + block].astype(jnp.bfloat16)
    logits = lax.dot_general(
        normed, router_ref[...], (((1,), (1,)), ((), ())), preferred_element_type=jnp.float32
    )
    lane = lax.broadcasted_iota(jnp.int32, logits.shape, 1)
    one, two = choice_ref[:, 0:1], choice_ref[:, 1:2]
    group = one // (experts // groups)

    def pick(mask, array):
        return jnp.sum(jnp.where(mask, array, jnp.float32(0.0)), axis=1, keepdims=True)

    raised = jnp.exp(logits)
    in_groups = jnp.logical_and(lane >= experts, lane < experts + groups)
    group_prob = pick(lane == experts + group, raised) / pick(in_groups, raised)
    first = jnp.exp(pick(lane == one, logits))
    second = jnp.exp(pick(lane == two, logits))
    both = first + second
    mix_ref[...] = jnp.where(
        lane == 0, group_prob * first / both, jnp.where(lane == 1, group_prob * second / both, 0.0)
    )


def experts_body(rows_ref, gate_ref, up_ref, down_ref, out_ref):
    rows = rows_ref[...]
    gate = jnp.dot(rows, gate_ref[...], preferred_element_type=jnp.float32)
    up = jnp.dot(rows, up_ref[...], preferred_element_type=jnp.float32)
    hidden = (jax.nn.silu(gate) * up).astype(jnp.bfloat16)
    out_ref[...] = jnp.dot(hidden, down_ref[...], preferred_element_type=jnp.float32).astype(
        jnp.bfloat16
    )


def mix_body(state_ref, first_ref, second_ref, mix_ref, *refs):
    returned_refs, out_ref = refs[:-1], refs[-1]
    returned = jnp.concatenate([returned[...] for returned in returned_refs], axis=0)
    first = jnp.dot(first_ref[...], returned, preferred_element_type=jnp.float32)
    second = jnp.dot(second_ref[...], returned, preferred_element_type=jnp.float32)
    mixture = mix_ref[:, 0:1] * first + mix_ref[:, 1:2] * second
    out_ref[...] = (state_ref[...].astype(jnp.float32) + mixture).astype(jnp.bfloat16)


def swap(array, dz=0, dc=0):
    flip = dz * 2 + dc
    return lax.ppermute(array, ("sp", "tp"), [(i, i ^ flip) for i in range(256)])


def cross(array, by, turn):
    pairs = [(i, i ^ (by * (16 if (i & 1) == turn else 64))) for i in range(256)]
    return lax.ppermute(array, ("sp", "tp"), pairs)


def role_of(core, y, x):
    return core ^ (x & 1) ^ (y & 1)


def deal(array, by, turn):
    pairs = []
    for i in range(256):
        along_x = role_of(i & 1, i >> 6, i >> 4 & 3) == turn
        pairs.append((i, i ^ (by * (16 if along_x else 64)) ^ (by & 1)))
    return lax.ppermute(array, ("sp", "tp"), pairs)


def shifted(array, axis, by):
    count = lax.axis_size(axis)
    pairs = [(i, i + by) for i in range(count) if 0 <= i + by < count]
    return lax.ppermute(array, axis, pairs)


def body(
    conv_value,
    conv_gate,
    doc_ids,
    conv_kernel,
    norm_gain_conv,
    norm_bias_conv,
    proj_weight,
    residual,
    norm_gain_moe,
    group_router,
    expert_router,
    routing,
    expert_gate_w,
    expert_up_w,
    expert_down_w,
):
    tokens, lanes = conv_value.shape
    rim = conv_kernel.shape[0] - 1
    count, width = residual.shape
    groups, experts = group_router.shape[1], expert_router.shape[1]
    slots = 2 * count
    capacity = slots // experts

    sp, tp = lax.axis_index("sp"), lax.axis_index("tp")
    z, core, y, x = tp >> 1, tp & 1, sp >> 2, sp & 3
    u, v = jnp.where(core == 0, x, y), jnp.where(core == 0, y, x)
    place = jnp.stack([z, core, v, u, sp, role_of(core, y, x)]).astype(jnp.int32)
    depth = proj_weight.shape[0]

    message = pl.pallas_call(
        rim_body,
        in_specs=[VMEM, VMEM, SMEM],
        out_specs=VMEM,
        out_shape=jax.ShapeDtypeStruct((64, lanes), jnp.bfloat16),
        compiler_params=params(8),
        name="tail",
    )(conv_value, conv_gate, doc_ids)
    came = shifted(message, "sp", 1)

    held = lax.dynamic_slice_in_dim(proj_weight, (v * 4 + u) * 128, 128, axis=1)[None]
    for bit in (4, 2, 1):
        other = swap(held, dz=bit)
        held = jnp.concatenate([held, other], axis=0)
    near = [held]
    for d in NEAR[1:]:
        near.append(cross(held, d, 0))
    low, high = (jnp.stack([part[at : at + 4] for part in near]) for at in (0, 4))
    low_1 = cross(low, 1, 1)
    high_3 = cross(high, 3, 1)
    low_32 = cross(jnp.stack([low, low_1]), 3, 1)
    high_12 = cross(jnp.stack([high, high_3]), 1, 1)
    pieces = [low, low_1, low_32, high, high_3, high_12]

    rim_values, rim_ids = came[:32], came[64 - rim :, 0].astype(jnp.int32)
    padded_ids = jnp.concatenate([rim_ids, doc_ids], axis=0)
    bounds = jnp.arange(24, dtype=jnp.int32)
    starts = jnp.sum((padded_ids[None, :] < bounds[:, None]).astype(jnp.int32), axis=1)
    tiles = doc_ids.reshape(8, tokens // 8)
    edges = jnp.stack([tiles[:, 0], tiles[:, -1]])
    convolved = convolve_tokens(
        place, starts, edges, conv_value, conv_gate, rim_values, conv_kernel, 8
    )
    raw = []
    for d in ORDER:
        raw.append(swap(convolved[d], dz=d) if d else convolved[d])

    spread, first_pick, second_pick, choice = pl.pallas_call(
        functools.partial(slots_body, capacity),
        in_specs=[SMEM, VMEM],
        out_specs=[VMEM] * 4,
        out_shape=[
            jax.ShapeDtypeStruct((slots, count), jnp.bfloat16),
            jax.ShapeDtypeStruct((count, slots), jnp.bfloat16),
            jax.ShapeDtypeStruct((count, slots), jnp.bfloat16),
            jax.ShapeDtypeStruct((count, 128), jnp.int32),
        ],
        compiler_params=params(8),
        name="slots",
    )(place, routing.T)
    routers = jnp.concatenate(
        [
            expert_router.T,
            group_router.T,
            jnp.zeros((32 - experts - groups, width), jnp.bfloat16),
        ],
        axis=0,
    )
    rows = 2 * count
    mine = pl.pallas_call(
        stats_body,
        in_specs=[VMEM] * 8,
        out_specs=VMEM,
        out_shape=jax.ShapeDtypeStruct((rows, lanes), jnp.float32),
        compiler_params=params(8),
        name="stats",
    )(*raw)
    other = swap(mine, dc=1)
    active = pl.pallas_call(
        functools.partial(activate_body, ORDER),
        in_specs=[SMEM] + [VMEM] * 12,
        out_specs=VMEM,
        out_shape=jax.ShapeDtypeStruct((rows, 8 * lanes), jnp.bfloat16),
        compiler_params=params(8),
        name="activate",
    )(
        place,
        mine,
        other,
        norm_gain_conv.reshape(-1, 1, lanes),
        norm_bias_conv.reshape(-1, 1, lanes),
        *raw,
    )
    kept, given = pl.pallas_call(
        partial_body,
        in_specs=[SMEM, VMEM] + [pl.BlockSpec(memory_space=pltpu.HBM)] * 6,
        out_specs=[VMEM] * 2,
        out_shape=[
            jax.ShapeDtypeStruct((count, width), jnp.float32),
            jax.ShapeDtypeStruct((count, width), jnp.bfloat16),
        ],
        scratch_shapes=[
            pltpu.VMEM((4, 8, depth, width // 4), jnp.bfloat16),
            pltpu.SemaphoreType.DMA((32,)),
        ],
        compiler_params=params(24),
        name="partial",
    )(place, active, *pieces)
    block = slots // 4
    state, mix, *outgoing = pl.pallas_call(
        functools.partial(state_body, groups, experts),
        in_specs=[VMEM] * 7,
        out_specs=[VMEM] * 6,
        out_shape=[
            jax.ShapeDtypeStruct((count, width), jnp.bfloat16),
            jax.ShapeDtypeStruct((count, 32), jnp.float32),
        ]
        + [jax.ShapeDtypeStruct((block, width), jnp.bfloat16)] * 4,
        compiler_params=params(24),
        name="state",
    )(
        kept,
        swap(given, dc=1),
        residual,
        norm_gain_moe[None, :],
        routers,
        choice,
        spread,
    )

    def regrouped(blocks, which):
        return jnp.concatenate(
            [blocks[i][which * capacity : which * capacity + capacity] for i in range(4)], axis=0
        )

    passing = {0: outgoing[0]} | {d: deal(outgoing[d], d, 0) for d in NEAR[1:]}
    arrived = {d: regrouped(passing, d) for d in NEAR}
    arrived = {d: deal(arrived[d], d, 1) if d else arrived[d] for d in NEAR}
    results = {
        d: pl.pallas_call(
            experts_body,
            in_specs=[VMEM] * 4,
            out_specs=VMEM,
            out_shape=jax.ShapeDtypeStruct((block, width), jnp.bfloat16),
            compiler_params=params(16),
            name="experts",
        )(arrived[d], expert_gate_w[0], expert_up_w[0], expert_down_w[0])
        for d in NEAR
    }
    results = {d: deal(results[d], d, 1) if d else results[d] for d in NEAR}
    returned = {d: regrouped(results, d) for d in NEAR}
    returned = {d: deal(returned[d], d, 0) if d else returned[d] for d in NEAR}
    return pl.pallas_call(
        mix_body,
        in_specs=[VMEM] * 8,
        out_specs=VMEM,
        out_shape=jax.ShapeDtypeStruct((count, width), jnp.bfloat16),
        compiler_params=params(16),
        name="mix",
    )(state, first_pick, second_pick, mix, *[returned[d] for d in range(4)])


def solution(mesh):
    placed = (
        P("sp", "tp"),
        P("sp", "tp"),
        P("sp"),
        P(None, "tp"),
        P(),
        P(),
        P("tp", None),
        P(("sp", "tp"), None),
        P(),
        P(),
        P(),
        P(("sp", "tp"), None),
        P("sp", None, None),
        P("sp", None, None),
        P("sp", None, None),
    )

    return jax.shard_map(
        body, mesh=mesh, in_specs=placed, out_specs=P(("sp", "tp"), None), check_vma=False
    )
```

```python
import functools

import jax
import jax.numpy as jnp
from jax import lax
from jax.experimental import pallas as pl
from jax.experimental.pallas import tpu as pltpu
from jax.sharding import PartitionSpec as P


epsilon = 1e-06
CHUNK = 64
ORDER = (0, 4, 2, 6, 1, 5, 3, 7)
NEAR = (0, 1, 3, 2)
VMEM = pl.BlockSpec(memory_space=pltpu.VMEM)
SMEM = pl.BlockSpec(memory_space=pltpu.SMEM)


def params(mib):
    return pltpu.CompilerParams(vmem_limit_bytes=mib * 1024 * 1024)


def conv_kernel_body(place_ref, ids_ref, ids_grid_ref, gated_ref, rim_ref, kernel_ref, *refs):
    outs, (taps, rows, masked, total) = refs[:-4], refs[-4:]
    tile, lanes = outs[0].shape
    tap_count = kernel_ref.shape[0]
    kernel = kernel_ref[...].astype(jnp.float32)
    for tap in range(tap_count):
        taps[8 * tap : 8 * tap + 8, :] = jnp.broadcast_to(kernel[tap : tap + 1, :], (8, lanes))
    rim_ids = rim_ref[32:64, :].astype(jnp.float32)
    rim_row = lax.broadcasted_iota(jnp.int32, rim_ids.shape, 0)
    rim_first = jnp.max(jnp.where(rim_row == 2, rim_ids, jnp.float32(0.0))).astype(jnp.int32)

    def begins(doc):
        own = jnp.sum(jnp.where(ids_grid_ref[...] < doc, jnp.float32(1.0), jnp.float32(0.0)))
        earlier = jnp.logical_and(rim_row >= 2, rim_ids < doc.astype(jnp.float32))
        before = jnp.sum(jnp.where(earlier, jnp.float32(1.0), jnp.float32(0.0)))
        return (own + before * jnp.float32(1.0 / lanes)).astype(jnp.int32)

    def convolve(source, at):
        acc = jnp.zeros((CHUNK // 8, 8, lanes), jnp.float32)
        for tap in range(tap_count):
            window = source[at + 2 + tap : at + 2 + tap + CHUNK, :].reshape(CHUNK // 8, 8, lanes)
            acc = acc + window * taps[8 * tap : 8 * tap + 8, :][None]
        return acc.reshape(CHUNK, lanes)

    def one_tile(step, carry):
        at_tile = step ^ place_ref[0]
        base = pl.multiple_of(at_tile * tile, tile)
        rows[32:, :] = gated_ref[pl.ds(base, tile), :].astype(jnp.float32)

        @pl.when(at_tile == 0)
        def _():
            rows[0:32, :] = rim_ref[0:32, :].astype(jnp.float32)

        @pl.when(at_tile > 0)
        def _():
            halo = pl.ds(pl.multiple_of(jnp.maximum(base - 32, 0), 32), 32)
            rows[0:32, :] = gated_ref[halo, :].astype(jnp.float32)

        def oldest(at):
            reach = base + at - 30
            return jnp.where(reach < 0, rim_first, ids_ref[jnp.maximum(reach, 0)])

        for at in range(0, tile, CHUNK):

            @pl.when(oldest(at) == ids_ref[base + at + CHUNK - 1])
            def _(at=at):
                total[at : at + CHUNK, :] = convolve(rows, at)

        def one_chunk(chunk, carry):
            at = pl.multiple_of(chunk * CHUNK, CHUNK)
            low, high = ids_ref[base + at], ids_ref[base + at + CHUNK - 1]

            @pl.when(oldest(at) != high)
            def _():
                total[pl.ds(at, CHUNK), :] = jnp.zeros((CHUNK, lanes), jnp.float32)

                def one_document(doc, carry):
                    first = begins(doc) - base - at + 2
                    last = begins(doc + 1) - base - at + 2
                    position = lax.broadcasted_iota(jnp.int32, masked.shape, 0)
                    masked[...] = jnp.where(
                        jnp.logical_and(position >= first, position < last),
                        rows[pl.ds(at, CHUNK + 32), :],
                        jnp.float32(0.0),
                    )
                    place = lax.broadcasted_iota(jnp.int32, (CHUNK, lanes), 0) + 32
                    inside = jnp.logical_and(place >= first, place < last)
                    total[pl.ds(at, CHUNK), :] += jnp.where(
                        inside, convolve(masked, 0), jnp.float32(0.0)
                    )
                    return carry

                lax.fori_loop(low, high + 1, one_document, 0)

            return carry

        lax.fori_loop(0, tile // CHUNK, one_chunk, 0)
        for slot, out in enumerate(outs):

            @pl.when(step == slot)
            def _(out=out):
                out[...] = total[...].astype(out.dtype)

        return carry

    lax.fori_loop(0, len(outs), one_tile, 0)


def convolve_tokens(place, ids, gated, rim, kernel, parts):
    tokens, lanes = gated.shape
    taps = kernel.shape[0]
    tile = tokens // parts
    return pl.pallas_call(
        conv_kernel_body,
        in_specs=[SMEM] * 2 + [VMEM] * 4,
        out_specs=[VMEM] * parts,
        scratch_shapes=[
            pltpu.VMEM((8 * taps, lanes), jnp.float32),
            pltpu.VMEM((tile + 32, lanes), jnp.float32),
            pltpu.VMEM((CHUNK + 32, lanes), jnp.float32),
            pltpu.VMEM((tile, lanes), jnp.float32),
        ],
        out_shape=[jax.ShapeDtypeStruct((tile, lanes), jnp.bfloat16)] * parts,
        compiler_params=params(12),
        name="gated_conv",
    )(place, ids, ids.reshape(-1, 128), gated, rim, kernel)


def slots_body(capacity, routing_ref, spread_ref, first_ref, second_ref, choice_ref):
    count = routing_ref.shape[1]
    slots = spread_ref.shape[0]
    row = lax.broadcasted_iota(jnp.int32, (count, count), 0)
    column = lax.broadcasted_iota(jnp.int32, (count, count), 1)

    def ones(mask):
        return jnp.where(mask, jnp.float32(1.0), jnp.float32(0.0))

    sub = lax.broadcasted_iota(jnp.int32, (16, count), 0)
    one, two = routing_ref[0:1, :], routing_ref[1:2, :]
    named = jnp.logical_or(sub == one, sub == two)
    before = jnp.dot(
        ones(named).astype(jnp.bfloat16),
        ones(row < column).astype(jnp.bfloat16),
        preferred_element_type=jnp.float32,
    )
    slot = lax.broadcasted_iota(jnp.int32, (slots, count), 0)
    targets = []
    for chosen in (one, two):
        position = jnp.sum(jnp.where(sub == chosen, before, 0.0), axis=0, keepdims=True)
        targets.append(chosen * capacity + position.astype(jnp.int32))
    spread_ref[...] = ones(jnp.logical_or(slot == targets[0], slot == targets[1])).astype(
        jnp.bfloat16
    )

    def upright(line):
        turned = jnp.sum(
            jnp.where(row == column, line.astype(jnp.float32), 0.0), axis=1, keepdims=True
        )
        return turned.astype(jnp.int32)

    slot = lax.broadcasted_iota(jnp.int32, (count, slots), 1)
    for target, out in zip(targets, (first_ref, second_ref), strict=True):
        out[...] = ones(slot == upright(target)).astype(jnp.bfloat16)
    lane = lax.broadcasted_iota(jnp.int32, choice_ref.shape, 1)
    choice_ref[...] = jnp.where(lane == 0, upright(one), upright(two))


def stats_body(*refs):
    raw_refs, out_ref = refs[:-1], refs[-1]
    count, lanes = raw_refs[0].shape
    summed = jnp.zeros((count, lanes), jnp.float32)
    for raw in raw_refs:
        summed = summed + raw[...].astype(jnp.float32)
    average = jnp.sum(summed, axis=1, keepdims=True) * jnp.float32(1.0 / (lanes * len(raw_refs)))
    squares = jnp.zeros((count, lanes), jnp.float32)
    for raw in raw_refs:
        centered = raw[...].astype(jnp.float32) - average
        squares = squares + centered * centered
    squares = jnp.sum(squares, axis=1, keepdims=True)
    lane = lax.broadcasted_iota(jnp.int32, (count, lanes), 1)
    out_ref[...] = jnp.where(lane == 0, average, squares)


def activate_body(order, place_ref, mine_ref, other_ref, gain_ref, bias_ref, *refs):
    raw_refs, out_ref = refs[:-1], refs[-1]
    rows, lanes = raw_refs[0].shape
    count = rows // 2
    half = lanes * len(raw_refs)
    core = place_ref[1]
    for block in range(2):
        at = pl.ds(pl.multiple_of((core ^ block) * count, count), count)
        to = slice(block * count, block * count + count)
        mine, other = mine_ref[at, :], other_ref[at, :]
        average = (mine[:, 0:1] + other[:, 0:1]) * jnp.float32(0.5)
        apart = mine[:, 0:1] - other[:, 0:1]
        spread = mine[:, 1:2] + other[:, 1:2] + apart * apart * jnp.float32(half / 2)
        scale = lax.rsqrt(spread * jnp.float32(0.5 / half) + epsilon)
        for slot, raw in enumerate(raw_refs):
            part = 2 * (place_ref[0] ^ order[slot]) + core
            value = (raw[at, :].astype(jnp.float32) - average) * scale * gain_ref[part] + bias_ref[
                part
            ]
            out_ref[to, slot * lanes : slot * lanes + lanes] = jax.nn.silu(value).astype(
                jnp.bfloat16
            )


def partial_body(
    place_ref,
    active_ref,
    low_ref,
    low_1_ref,
    low_32_ref,
    high_ref,
    high_3_ref,
    high_12_ref,
    mine_ref,
    other_ref,
    weight,
    sems,
):
    _, slots, depth, group = weight.shape
    count = mine_ref.shape[0]
    v, u = place_ref[2], place_ref[3]
    sources = (
        (0, low_ref, high_ref),
        (1, low_1_ref, high_12_ref.at[0]),
        (3, low_32_ref.at[0], high_3_ref),
        (2, low_32_ref.at[1], high_12_ref.at[1]),
    )
    copies = []
    for number, (_, *halves) in enumerate(sources):
        for side, half in enumerate(halves):
            for nth, near in enumerate(NEAR):
                copy = pltpu.make_async_copy(
                    half.at[nth],
                    weight.at[
                        number,
                        pl.ds(4 * side, 4),
                        :,
                        pl.ds(pl.multiple_of((u ^ near) * 128, 128), 128),
                    ],
                    sems.at[8 * number + 4 * side + nth],
                )
                copy.start()
                copies.append(copy)
    for number, (far, *_) in enumerate(sources):
        for nth in range(8):
            copies[8 * number + nth].wait()
        product = jnp.dot(
            active_ref[...],
            weight[number].reshape(slots * depth, group),
            preferred_element_type=jnp.float32,
        )
        to = pl.ds(pl.multiple_of((v ^ far) * group, group), group)
        mine_ref[:, to] = product[:count]
        other_ref[:, to] = product[count:].astype(other_ref.dtype)


def state_body(
    groups,
    experts,
    mine_ref,
    other_ref,
    residual_ref,
    gain_moe_ref,
    router_ref,
    choice_ref,
    spread_ref,
    state_ref,
    mix_ref,
    outgoing_ref,
):
    projected = (
        residual_ref[...].astype(jnp.float32) + mine_ref[...] + other_ref[...].astype(jnp.float32)
    )
    state = projected.astype(jnp.bfloat16)
    state_ref[...] = state
    state = state.astype(jnp.float32)
    power = jnp.mean(state * state, axis=1, keepdims=True)
    normed = (state * lax.rsqrt(power + epsilon) * gain_moe_ref[...]).astype(jnp.bfloat16)
    outgoing_ref[...] = jnp.dot(
        spread_ref[...], normed, preferred_element_type=jnp.float32
    ).astype(jnp.bfloat16)
    logits = lax.dot_general(
        normed, router_ref[...], (((1,), (1,)), ((), ())), preferred_element_type=jnp.float32
    )
    lane = lax.broadcasted_iota(jnp.int32, logits.shape, 1)
    one, two = choice_ref[:, 0:1], choice_ref[:, 1:2]
    group = one // (experts // groups)

    def pick(mask, array):
        return jnp.sum(jnp.where(mask, array, jnp.float32(0.0)), axis=1, keepdims=True)

    raised = jnp.exp(logits)
    in_groups = jnp.logical_and(lane >= experts, lane < experts + groups)
    group_prob = pick(lane == experts + group, raised) / pick(in_groups, raised)
    first = jnp.exp(pick(lane == one, logits))
    second = jnp.exp(pick(lane == two, logits))
    both = first + second
    mix_ref[...] = jnp.where(
        lane == 0, group_prob * first / both, jnp.where(lane == 1, group_prob * second / both, 0.0)
    )


def experts_body(rows_ref, gate_ref, up_ref, down_ref, out_ref):
    rows = rows_ref[...]
    gate = jnp.dot(rows, gate_ref[...], preferred_element_type=jnp.float32)
    up = jnp.dot(rows, up_ref[...], preferred_element_type=jnp.float32)
    hidden = (jax.nn.silu(gate) * up).astype(jnp.bfloat16)
    out_ref[...] = jnp.dot(hidden, down_ref[...], preferred_element_type=jnp.float32).astype(
        jnp.bfloat16
    )


def mix_body(state_ref, first_ref, second_ref, mix_ref, returned_ref, out_ref):
    returned = returned_ref[...]
    first = jnp.dot(first_ref[...], returned, preferred_element_type=jnp.float32)
    second = jnp.dot(second_ref[...], returned, preferred_element_type=jnp.float32)
    mixture = mix_ref[:, 0:1] * first + mix_ref[:, 1:2] * second
    out_ref[...] = (state_ref[...].astype(jnp.float32) + mixture).astype(jnp.bfloat16)


def swap(array, dz=0, dc=0):
    flip = dz * 2 + dc
    return lax.ppermute(array, ("sp", "tp"), [(i, i ^ flip) for i in range(256)])


def cross(array, by, turn):
    pairs = [(i, i ^ (by * (16 if (i & 1) == turn else 64))) for i in range(256)]
    return lax.ppermute(array, ("sp", "tp"), pairs)


def shifted(array, axis, by):
    count = lax.axis_size(axis)
    pairs = [(i, i + by) for i in range(count) if 0 <= i + by < count]
    return lax.ppermute(array, axis, pairs)


def body(
    conv_value,
    conv_gate,
    doc_ids,
    conv_kernel,
    norm_gain_conv,
    norm_bias_conv,
    proj_weight,
    residual,
    norm_gain_moe,
    group_router,
    expert_router,
    routing,
    expert_gate_w,
    expert_up_w,
    expert_down_w,
):
    tokens, lanes = conv_value.shape
    count, width = residual.shape
    groups, experts = group_router.shape[1], expert_router.shape[1]
    slots = 2 * count
    capacity = slots // experts

    sp, tp = lax.axis_index("sp"), lax.axis_index("tp")
    z, core, y, x = tp >> 1, tp & 1, sp >> 2, sp & 3
    u, v = jnp.where(core == 0, x, y), jnp.where(core == 0, y, x)
    place = jnp.stack([z, core, v, u]).astype(jnp.int32)
    depth = proj_weight.shape[0]

    gated = (
        conv_value.astype(jnp.float32) * jax.nn.sigmoid(conv_gate.astype(jnp.float32))
    ).astype(jnp.bfloat16)
    tail = slice(tokens - 32, tokens)
    tail_ids = jnp.broadcast_to(doc_ids[tail][:, None], (32, lanes)).astype(jnp.bfloat16)
    message = jnp.concatenate([gated[tail], tail_ids], axis=0)
    came = shifted(message, "sp", 1)

    held = lax.dynamic_slice_in_dim(proj_weight, (v * 4 + u) * 128, 128, axis=1)[None]
    for bit in (4, 2, 1):
        other = swap(held, dz=bit)
        held = jnp.concatenate([held, other], axis=0)
    near = [held]
    for d in NEAR[1:]:
        near.append(cross(held, d, 0))
    low, high = (jnp.stack([part[at : at + 4] for part in near]) for at in (0, 4))
    low_1 = cross(low, 1, 1)
    high_3 = cross(high, 3, 1)
    low_32 = cross(jnp.stack([low, low_1]), 3, 1)
    high_12 = cross(jnp.stack([high, high_3]), 1, 1)
    pieces = [low, low_1, low_32, high, high_3, high_12]

    convolved = convolve_tokens(place, doc_ids, gated, came, conv_kernel, 8)
    raw = []
    for d in ORDER:
        raw.append(swap(convolved[d], dz=d) if d else convolved[d])

    spread, first_pick, second_pick, choice = pl.pallas_call(
        functools.partial(slots_body, capacity),
        in_specs=[VMEM],
        out_specs=[VMEM] * 4,
        out_shape=[
            jax.ShapeDtypeStruct((slots, count), jnp.bfloat16),
            jax.ShapeDtypeStruct((count, slots), jnp.bfloat16),
            jax.ShapeDtypeStruct((count, slots), jnp.bfloat16),
            jax.ShapeDtypeStruct((count, 128), jnp.int32),
        ],
        compiler_params=params(8),
        name="slots",
    )(routing.T)
    routers = jnp.concatenate(
        [
            expert_router.T,
            group_router.T,
            jnp.zeros((32 - experts - groups, width), jnp.bfloat16),
        ],
        axis=0,
    )
    rows = 2 * count
    mine = pl.pallas_call(
        stats_body,
        in_specs=[VMEM] * 8,
        out_specs=VMEM,
        out_shape=jax.ShapeDtypeStruct((rows, lanes), jnp.float32),
        compiler_params=params(8),
        name="stats",
    )(*raw)
    other = swap(mine, dc=1)
    active = pl.pallas_call(
        functools.partial(activate_body, ORDER),
        in_specs=[SMEM] + [VMEM] * 12,
        out_specs=VMEM,
        out_shape=jax.ShapeDtypeStruct((rows, 8 * lanes), jnp.bfloat16),
        compiler_params=params(8),
        name="activate",
    )(
        place,
        mine,
        other,
        norm_gain_conv.reshape(-1, 1, lanes),
        norm_bias_conv.reshape(-1, 1, lanes),
        *raw,
    )
    kept, given = pl.pallas_call(
        partial_body,
        in_specs=[SMEM, VMEM] + [pl.BlockSpec(memory_space=pltpu.HBM)] * 6,
        out_specs=[VMEM] * 2,
        out_shape=[
            jax.ShapeDtypeStruct((count, width), jnp.float32),
            jax.ShapeDtypeStruct((count, width), jnp.bfloat16),
        ],
        scratch_shapes=[
            pltpu.VMEM((4, 8, depth, width // 4), jnp.bfloat16),
            pltpu.SemaphoreType.DMA((32,)),
        ],
        compiler_params=params(24),
        name="partial",
    )(place, active, *pieces)
    state, mix, outgoing = pl.pallas_call(
        functools.partial(state_body, groups, experts),
        in_specs=[VMEM] * 7,
        out_specs=[VMEM] * 3,
        out_shape=[
            jax.ShapeDtypeStruct((count, width), jnp.bfloat16),
            jax.ShapeDtypeStruct((count, 32), jnp.float32),
            jax.ShapeDtypeStruct((slots, width), jnp.bfloat16),
        ],
        compiler_params=params(24),
        name="state",
    )(
        kept,
        swap(given, dc=1),
        residual,
        norm_gain_moe[None, :],
        routers,
        choice,
        spread,
    )

    def exchanged(rows):
        blocks = rows.reshape(experts, capacity, width)
        return lax.all_to_all(blocks, "sp", split_axis=0, concat_axis=0, tiled=True).reshape(
            slots, width
        )

    result = pl.pallas_call(
        experts_body,
        in_specs=[VMEM] * 4,
        out_specs=VMEM,
        out_shape=jax.ShapeDtypeStruct((slots, width), jnp.bfloat16),
        compiler_params=params(20),
        name="experts",
    )(exchanged(outgoing), expert_gate_w[0], expert_up_w[0], expert_down_w[0])
    return pl.pallas_call(
        mix_body,
        in_specs=[VMEM] * 5,
        out_specs=VMEM,
        out_shape=jax.ShapeDtypeStruct((count, width), jnp.bfloat16),
        compiler_params=params(16),
        name="mix",
    )(state, first_pick, second_pick, mix, exchanged(result))


def solution(mesh):
    placed = (
        P("sp", "tp"),
        P("sp", "tp"),
        P("sp"),
        P(None, "tp"),
        P(),
        P(),
        P("tp", None),
        P(("sp", "tp"), None),
        P(),
        P(),
        P(),
        P(("sp", "tp"), None),
        P("sp", None, None),
        P("sp", None, None),
        P("sp", None, None),
    )

    return jax.shard_map(
        body, mesh=mesh, in_specs=placed, out_specs=P(("sp", "tp"), None), check_vma=False
    )
```

```python
import functools

import jax
import jax.numpy as jnp
from jax import lax
from jax.experimental import pallas as pl
from jax.experimental.pallas import tpu as pltpu
from jax.sharding import PartitionSpec as P


epsilon = 1e-06
CHUNK = 64
ORDER = (0, 4, 2, 6, 1, 5, 3, 7)
NEAR = (0, 1, 3, 2)
VMEM = pl.BlockSpec(memory_space=pltpu.VMEM)
SMEM = pl.BlockSpec(memory_space=pltpu.SMEM)


def params(mib):
    return pltpu.CompilerParams(vmem_limit_bytes=mib * 1024 * 1024)


def conv_kernel_body(begin, ids_ref, ids_grid_ref, gated_ref, kernel_ref, *refs):
    rims, (out_ref, taps, rows, masked, total) = refs[:-5], refs[-5:]
    count, tile, lanes = out_ref.shape
    tap_count = kernel_ref.shape[0]
    kernel = kernel_ref[...].astype(jnp.float32)
    for tap in range(tap_count):
        taps[8 * tap : 8 * tap + 8, :] = jnp.broadcast_to(kernel[tap : tap + 1, :], (8, lanes))
    rim_row = lax.broadcasted_iota(jnp.int32, (32, lanes), 0)
    if begin == 0:
        rim_ids = rims[0][32:64, :].astype(jnp.float32)
        rim_first = jnp.max(jnp.where(rim_row == 2, rim_ids, jnp.float32(0.0))).astype(jnp.int32)

    def begins(doc):
        own = jnp.sum(jnp.where(ids_grid_ref[...] < doc, jnp.float32(1.0), jnp.float32(0.0)))
        if begin > 0:
            return own.astype(jnp.int32) + 30
        earlier = jnp.logical_and(rim_row >= 2, rim_ids < doc.astype(jnp.float32))
        before = jnp.sum(jnp.where(earlier, jnp.float32(1.0), jnp.float32(0.0)))
        return (own + before * jnp.float32(1.0 / lanes)).astype(jnp.int32)

    def convolve(source, at):
        acc = jnp.zeros((CHUNK // 8, 8, lanes), jnp.float32)
        for tap in range(tap_count):
            window = source[at + 2 + tap : at + 2 + tap + CHUNK, :].reshape(CHUNK // 8, 8, lanes)
            acc = acc + window * taps[8 * tap : 8 * tap + 8, :][None]
        return acc.reshape(CHUNK, lanes)

    def one_tile(step, carry):
        base = pl.multiple_of((begin + step) * tile, tile)
        halo = pl.ds(pl.multiple_of(jnp.maximum(base - 32, 0), 32), 32)
        rows[32:, :] = gated_ref[pl.ds(base, tile), :].astype(jnp.float32)
        rows[0:32, :] = gated_ref[halo, :].astype(jnp.float32)
        if begin == 0:

            @pl.when(step == 0)
            def _():
                rows[0:32, :] = rims[0][0:32, :].astype(jnp.float32)

        def oldest(at):
            reach = base + at - 30
            if begin > 0:
                return ids_ref[reach]
            return jnp.where(reach < 0, rim_first, ids_ref[jnp.maximum(reach, 0)])

        for at in range(0, tile, CHUNK):

            @pl.when(oldest(at) == ids_ref[base + at + CHUNK - 1])
            def _(at=at):
                total[at : at + CHUNK, :] = convolve(rows, at)

        def one_chunk(chunk, carry):
            at = pl.multiple_of(chunk * CHUNK, CHUNK)
            low, high = ids_ref[base + at], ids_ref[base + at + CHUNK - 1]

            @pl.when(oldest(at) != high)
            def _():
                total[pl.ds(at, CHUNK), :] = jnp.zeros((CHUNK, lanes), jnp.float32)

                def one_document(doc, carry):
                    first = begins(doc) - base - at + 2
                    last = begins(doc + 1) - base - at + 2
                    position = lax.broadcasted_iota(jnp.int32, masked.shape, 0)
                    masked[...] = jnp.where(
                        jnp.logical_and(position >= first, position < last),
                        rows[pl.ds(at, CHUNK + 32), :],
                        jnp.float32(0.0),
                    )
                    place = lax.broadcasted_iota(jnp.int32, (CHUNK, lanes), 0) + 32
                    inside = jnp.logical_and(place >= first, place < last)
                    total[pl.ds(at, CHUNK), :] += jnp.where(
                        inside, convolve(masked, 0), jnp.float32(0.0)
                    )
                    return carry

                lax.fori_loop(low, high + 1, one_document, 0)

            return carry

        lax.fori_loop(0, tile // CHUNK, one_chunk, 0)
        out_ref[step] = total[...].astype(out_ref.dtype)
        return carry

    lax.fori_loop(0, count, one_tile, 0)


def convolve_tokens(begin, count, tile, ids, gated, kernel, *rims):
    lanes = gated.shape[1]
    taps = kernel.shape[0]
    return pl.pallas_call(
        functools.partial(conv_kernel_body, begin),
        in_specs=[SMEM] + [VMEM] * (3 + len(rims)),
        out_specs=VMEM,
        scratch_shapes=[
            pltpu.VMEM((8 * taps, lanes), jnp.float32),
            pltpu.VMEM((tile + 32, lanes), jnp.float32),
            pltpu.VMEM((CHUNK + 32, lanes), jnp.float32),
            pltpu.VMEM((tile, lanes), jnp.float32),
        ],
        out_shape=jax.ShapeDtypeStruct((count, tile, lanes), jnp.bfloat16),
        compiler_params=params(12),
        name="conv_head" if begin == 0 else "conv_rest",
    )(ids, ids.reshape(-1, 128), gated, kernel, *rims)


def slots_body(capacity, routing_ref, spread_ref, first_ref, second_ref, choice_ref):
    count = routing_ref.shape[1]
    slots = spread_ref.shape[0]
    row = lax.broadcasted_iota(jnp.int32, (count, count), 0)
    column = lax.broadcasted_iota(jnp.int32, (count, count), 1)

    def ones(mask):
        return jnp.where(mask, jnp.float32(1.0), jnp.float32(0.0))

    sub = lax.broadcasted_iota(jnp.int32, (16, count), 0)
    one, two = routing_ref[0:1, :], routing_ref[1:2, :]
    named = jnp.logical_or(sub == one, sub == two)
    before = jnp.dot(
        ones(named).astype(jnp.bfloat16),
        ones(row < column).astype(jnp.bfloat16),
        preferred_element_type=jnp.float32,
    )
    slot = lax.broadcasted_iota(jnp.int32, (slots, count), 0)
    targets = []
    for chosen in (one, two):
        position = jnp.sum(jnp.where(sub == chosen, before, 0.0), axis=0, keepdims=True)
        targets.append(chosen * capacity + position.astype(jnp.int32))
    spread_ref[...] = ones(jnp.logical_or(slot == targets[0], slot == targets[1])).astype(
        jnp.bfloat16
    )

    def upright(line):
        turned = jnp.sum(
            jnp.where(row == column, line.astype(jnp.float32), 0.0), axis=1, keepdims=True
        )
        return turned.astype(jnp.int32)

    slot = lax.broadcasted_iota(jnp.int32, (count, slots), 1)
    for target, out in zip(targets, (first_ref, second_ref), strict=True):
        out[...] = ones(slot == upright(target)).astype(jnp.bfloat16)
    lane = lax.broadcasted_iota(jnp.int32, choice_ref.shape, 1)
    choice_ref[...] = jnp.where(lane == 0, upright(one), upright(two))


def stats_body(*refs):
    raw_refs, out_ref = refs[:-1], refs[-1]
    count, lanes = raw_refs[0].shape
    summed = jnp.zeros((count, lanes), jnp.float32)
    for raw in raw_refs:
        summed = summed + raw[...].astype(jnp.float32)
    average = jnp.sum(summed, axis=1, keepdims=True) * jnp.float32(1.0 / (lanes * len(raw_refs)))
    squares = jnp.zeros((count, lanes), jnp.float32)
    for raw in raw_refs:
        centered = raw[...].astype(jnp.float32) - average
        squares = squares + centered * centered
    squares = jnp.sum(squares, axis=1, keepdims=True)
    lane = lax.broadcasted_iota(jnp.int32, (count, lanes), 1)
    out_ref[...] = jnp.where(lane == 0, average, squares)


def activate_body(order, place_ref, mine_ref, other_ref, gain_ref, bias_ref, *refs):
    raw_refs, out_ref = refs[:-1], refs[-1]
    rows, lanes = raw_refs[0].shape
    count = rows // 2
    half = lanes * len(raw_refs)
    core = place_ref[1]
    for block in range(2):
        at = pl.ds(pl.multiple_of((core ^ block) * count, count), count)
        to = slice(block * count, block * count + count)
        mine, other = mine_ref[at, :], other_ref[at, :]
        average = (mine[:, 0:1] + other[:, 0:1]) * jnp.float32(0.5)
        apart = mine[:, 0:1] - other[:, 0:1]
        spread = mine[:, 1:2] + other[:, 1:2] + apart * apart * jnp.float32(half / 2)
        scale = lax.rsqrt(spread * jnp.float32(0.5 / half) + epsilon)
        for slot, raw in enumerate(raw_refs):
            part = 2 * (place_ref[0] ^ order[slot]) + core
            value = (raw[at, :].astype(jnp.float32) - average) * scale * gain_ref[part] + bias_ref[
                part
            ]
            out_ref[to, slot * lanes : slot * lanes + lanes] = jax.nn.silu(value).astype(
                jnp.bfloat16
            )


def partial_body(
    place_ref,
    active_ref,
    low_ref,
    low_1_ref,
    low_32_ref,
    high_ref,
    high_3_ref,
    high_12_ref,
    mine_ref,
    other_ref,
):
    nears, slots, depth, lanes = low_ref.shape
    count = mine_ref.shape[0]
    v, u = place_ref[2], place_ref[3]
    sources = (
        (0, low_ref, high_ref),
        (1, low_1_ref, high_12_ref.at[0]),
        (3, low_32_ref.at[0], high_3_ref),
        (2, low_32_ref.at[1], high_12_ref.at[1]),
    )
    for far, *halves in sources:
        weight = jnp.concatenate(
            [
                jnp.concatenate(
                    [half[nth].reshape(slots * depth, lanes) for half in halves], axis=0
                )
                for nth in range(nears)
            ],
            axis=1,
        )
        product = jnp.dot(active_ref[...], weight, preferred_element_type=jnp.float32)
        for nth, near in enumerate(NEAR):
            piece = product[:, nth * lanes : nth * lanes + lanes]
            to = pl.ds(pl.multiple_of(((v ^ far) * nears + (u ^ near)) * lanes, lanes), lanes)
            mine_ref[:, to] = piece[:count]
            other_ref[:, to] = piece[count:].astype(other_ref.dtype)


def state_body(
    groups,
    experts,
    mine_ref,
    other_ref,
    residual_ref,
    gain_moe_ref,
    router_ref,
    choice_ref,
    spread_ref,
    state_ref,
    mix_ref,
    outgoing_ref,
):
    projected = (
        residual_ref[...].astype(jnp.float32) + mine_ref[...] + other_ref[...].astype(jnp.float32)
    )
    state = projected.astype(jnp.bfloat16)
    state_ref[...] = state
    state = state.astype(jnp.float32)
    power = jnp.mean(state * state, axis=1, keepdims=True)
    normed = (state * lax.rsqrt(power + epsilon) * gain_moe_ref[...]).astype(jnp.bfloat16)
    outgoing_ref[...] = jnp.dot(
        spread_ref[...], normed, preferred_element_type=jnp.float32
    ).astype(jnp.bfloat16)
    logits = lax.dot_general(
        normed, router_ref[...], (((1,), (1,)), ((), ())), preferred_element_type=jnp.float32
    )
    lane = lax.broadcasted_iota(jnp.int32, logits.shape, 1)
    one, two = choice_ref[:, 0:1], choice_ref[:, 1:2]
    group = one // (experts // groups)

    def pick(mask, array):
        return jnp.sum(jnp.where(mask, array, jnp.float32(0.0)), axis=1, keepdims=True)

    raised = jnp.exp(logits)
    in_groups = jnp.logical_and(lane >= experts, lane < experts + groups)
    group_prob = pick(lane == experts + group, raised) / pick(in_groups, raised)
    first = jnp.exp(pick(lane == one, logits))
    second = jnp.exp(pick(lane == two, logits))
    both = first + second
    mix_ref[...] = jnp.where(
        lane == 0, group_prob * first / both, jnp.where(lane == 1, group_prob * second / both, 0.0)
    )


def experts_body(rows_ref, gate_ref, up_ref, down_ref, out_ref):
    rows = rows_ref[...]
    gate = jnp.dot(rows, gate_ref[...], preferred_element_type=jnp.float32)
    up = jnp.dot(rows, up_ref[...], preferred_element_type=jnp.float32)
    hidden = (jax.nn.silu(gate) * up).astype(jnp.bfloat16)
    out_ref[...] = jnp.dot(hidden, down_ref[...], preferred_element_type=jnp.float32).astype(
        jnp.bfloat16
    )


def mix_body(state_ref, first_ref, second_ref, mix_ref, returned_ref, out_ref):
    returned = returned_ref[...]
    first = jnp.dot(first_ref[...], returned, preferred_element_type=jnp.float32)
    second = jnp.dot(second_ref[...], returned, preferred_element_type=jnp.float32)
    mixture = mix_ref[:, 0:1] * first + mix_ref[:, 1:2] * second
    out_ref[...] = (state_ref[...].astype(jnp.float32) + mixture).astype(jnp.bfloat16)


def swap(array, dz=0, dc=0):
    flip = dz * 2 + dc
    return lax.ppermute(array, ("sp", "tp"), [(i, i ^ flip) for i in range(256)])


def cross(array, by, turn):
    pairs = [(i, i ^ (by * (16 if (i & 1) == turn else 64))) for i in range(256)]
    return lax.ppermute(array, ("sp", "tp"), pairs)


def shifted(array, axis, by):
    count = lax.axis_size(axis)
    pairs = [(i, i + by) for i in range(count) if 0 <= i + by < count]
    return lax.ppermute(array, axis, pairs)


def body(
    conv_value,
    conv_gate,
    doc_ids,
    conv_kernel,
    norm_gain_conv,
    norm_bias_conv,
    proj_weight,
    residual,
    norm_gain_moe,
    group_router,
    expert_router,
    routing,
    expert_gate_w,
    expert_up_w,
    expert_down_w,
):
    tokens, lanes = conv_value.shape
    count, width = residual.shape
    groups, experts = group_router.shape[1], expert_router.shape[1]
    slots = 2 * count
    capacity = slots // experts

    sp, tp = lax.axis_index("sp"), lax.axis_index("tp")
    z, core, y, x = tp >> 1, tp & 1, sp >> 2, sp & 3
    u, v = jnp.where(core == 0, x, y), jnp.where(core == 0, y, x)
    place = jnp.stack([z, core, v, u]).astype(jnp.int32)

    gated = (
        conv_value.astype(jnp.float32) * jax.nn.sigmoid(conv_gate.astype(jnp.float32))
    ).astype(jnp.bfloat16)
    tail = slice(tokens - 32, tokens)
    tail_ids = jnp.broadcast_to(doc_ids[tail][:, None], (32, lanes)).astype(jnp.bfloat16)
    message = jnp.concatenate([gated[tail], tail_ids], axis=0)
    came = shifted(message, "sp", 1)

    held = lax.dynamic_slice_in_dim(proj_weight, (v * 4 + u) * 128, 128, axis=1)[None]
    for bit in (4, 2, 1):
        other = swap(held, dz=bit)
        held = jnp.concatenate([held, other], axis=0)
    near = [held]
    for d in NEAR[1:]:
        near.append(cross(held, d, 0))
    low, high = (jnp.stack([part[at : at + 4] for part in near]) for at in (0, 4))
    low_1 = cross(low, 1, 1)
    high_3 = cross(high, 3, 1)
    low_32 = cross(jnp.stack([low, low_1]), 3, 1)
    high_12 = cross(jnp.stack([high, high_3]), 1, 1)
    pieces = [low, low_1, low_32, high, high_3, high_12]

    tile = 2 * count
    rest = convolve_tokens(4, 4, tile, doc_ids, gated, conv_kernel)
    head = convolve_tokens(0, 4, tile, doc_ids, gated, conv_kernel, came)
    convolved = lax.optimization_barrier(jnp.concatenate([head, rest], axis=0))
    raw = []
    for d in ORDER:
        part = lax.dynamic_index_in_dim(convolved, z ^ d, 0, keepdims=False)
        raw.append(swap(part, dz=d) if d else part)

    spread, first_pick, second_pick, choice = pl.pallas_call(
        functools.partial(slots_body, capacity),
        in_specs=[VMEM],
        out_specs=[VMEM] * 4,
        out_shape=[
            jax.ShapeDtypeStruct((slots, count), jnp.bfloat16),
            jax.ShapeDtypeStruct((count, slots), jnp.bfloat16),
            jax.ShapeDtypeStruct((count, slots), jnp.bfloat16),
            jax.ShapeDtypeStruct((count, 128), jnp.int32),
        ],
        compiler_params=params(8),
        name="slots",
    )(routing.T)
    routers = jnp.concatenate(
        [
            expert_router.T,
            group_router.T,
            jnp.zeros((32 - experts - groups, width), jnp.bfloat16),
        ],
        axis=0,
    )
    rows = 2 * count
    mine = pl.pallas_call(
        stats_body,
        in_specs=[VMEM] * 8,
        out_specs=VMEM,
        out_shape=jax.ShapeDtypeStruct((rows, lanes), jnp.float32),
        compiler_params=params(8),
        name="stats",
    )(*raw)
    other = swap(mine, dc=1)
    active = pl.pallas_call(
        functools.partial(activate_body, ORDER),
        in_specs=[SMEM] + [VMEM] * 12,
        out_specs=VMEM,
        out_shape=jax.ShapeDtypeStruct((rows, 8 * lanes), jnp.bfloat16),
        compiler_params=params(8),
        name="activate",
    )(
        place,
        mine,
        other,
        norm_gain_conv.reshape(-1, 1, lanes),
        norm_bias_conv.reshape(-1, 1, lanes),
        *raw,
    )
    kept, given = pl.pallas_call(
        partial_body,
        in_specs=[SMEM] + [VMEM] * 7,
        out_specs=[VMEM] * 2,
        out_shape=[
            jax.ShapeDtypeStruct((count, width), jnp.float32),
            jax.ShapeDtypeStruct((count, width), jnp.bfloat16),
        ],
        compiler_params=params(24),
        name="partial",
    )(place, active, *pieces)
    state, mix, outgoing = pl.pallas_call(
        functools.partial(state_body, groups, experts),
        in_specs=[VMEM] * 7,
        out_specs=[VMEM] * 3,
        out_shape=[
            jax.ShapeDtypeStruct((count, width), jnp.bfloat16),
            jax.ShapeDtypeStruct((count, 32), jnp.float32),
            jax.ShapeDtypeStruct((slots, width), jnp.bfloat16),
        ],
        compiler_params=params(24),
        name="state",
    )(
        kept,
        swap(given, dc=1),
        residual,
        norm_gain_moe[None, :],
        routers,
        choice,
        spread,
    )

    def exchanged(rows):
        blocks = rows.reshape(experts, capacity, width)
        return lax.all_to_all(blocks, "sp", split_axis=0, concat_axis=0, tiled=True).reshape(
            slots, width
        )

    result = pl.pallas_call(
        experts_body,
        in_specs=[VMEM] * 4,
        out_specs=VMEM,
        out_shape=jax.ShapeDtypeStruct((slots, width), jnp.bfloat16),
        compiler_params=params(20),
        name="experts",
    )(exchanged(outgoing), expert_gate_w[0], expert_up_w[0], expert_down_w[0])
    return pl.pallas_call(
        mix_body,
        in_specs=[VMEM] * 5,
        out_specs=VMEM,
        out_shape=jax.ShapeDtypeStruct((count, width), jnp.bfloat16),
        compiler_params=params(16),
        name="mix",
    )(state, first_pick, second_pick, mix, exchanged(result))


def solution(mesh):
    placed = (
        P("sp", "tp"),
        P("sp", "tp"),
        P("sp"),
        P(None, "tp"),
        P(),
        P(),
        P("tp", None),
        P(("sp", "tp"), None),
        P(),
        P(),
        P(),
        P(("sp", "tp"), None),
        P("sp", None, None),
        P("sp", None, None),
        P("sp", None, None),
    )

    return jax.shard_map(
        body, mesh=mesh, in_specs=placed, out_specs=P(("sp", "tp"), None), check_vma=False
    )
```

```python
import functools

import jax
import jax.numpy as jnp
from jax import lax
from jax.experimental import pallas as pl
from jax.experimental.pallas import tpu as pltpu
from jax.sharding import PartitionSpec as P


epsilon = 1e-06
CHUNK = 64
ORDER = (0, 4, 2, 6, 1, 5, 3, 7)
NEAR = (0, 1, 3, 2)
VMEM = pl.BlockSpec(memory_space=pltpu.VMEM)
SMEM = pl.BlockSpec(memory_space=pltpu.SMEM)


def params(mib):
    return pltpu.CompilerParams(vmem_limit_bytes=mib * 1024 * 1024)


def conv_kernel_body(begin, ids_ref, ids_grid_ref, gated_ref, kernel_ref, *refs):
    rims, (out_ref, taps, rows, masked, total) = refs[:-5], refs[-5:]
    count, tile, lanes = out_ref.shape
    tap_count = kernel_ref.shape[0]
    kernel = kernel_ref[...].astype(jnp.float32)
    for tap in range(tap_count):
        taps[8 * tap : 8 * tap + 8, :] = jnp.broadcast_to(kernel[tap : tap + 1, :], (8, lanes))
    rim_row = lax.broadcasted_iota(jnp.int32, (32, lanes), 0)
    if begin == 0:
        rim_ids = rims[0][32:64, :].astype(jnp.float32)
        rim_first = jnp.max(jnp.where(rim_row == 2, rim_ids, jnp.float32(0.0))).astype(jnp.int32)

    def begins(doc):
        own = jnp.sum(jnp.where(ids_grid_ref[...] < doc, jnp.float32(1.0), jnp.float32(0.0)))
        if begin > 0:
            return own.astype(jnp.int32) + 30
        earlier = jnp.logical_and(rim_row >= 2, rim_ids < doc.astype(jnp.float32))
        before = jnp.sum(jnp.where(earlier, jnp.float32(1.0), jnp.float32(0.0)))
        return (own + before * jnp.float32(1.0 / lanes)).astype(jnp.int32)

    def convolve(source, at):
        acc = jnp.zeros((CHUNK // 8, 8, lanes), jnp.float32)
        for tap in range(tap_count):
            window = source[at + 2 + tap : at + 2 + tap + CHUNK, :].reshape(CHUNK // 8, 8, lanes)
            acc = acc + window * taps[8 * tap : 8 * tap + 8, :][None]
        return acc.reshape(CHUNK, lanes)

    def one_tile(step, carry):
        base = pl.multiple_of((begin + step) * tile, tile)
        halo = pl.ds(pl.multiple_of(jnp.maximum(base - 32, 0), 32), 32)
        rows[32:, :] = gated_ref[pl.ds(base, tile), :].astype(jnp.float32)
        rows[0:32, :] = gated_ref[halo, :].astype(jnp.float32)
        if begin == 0:

            @pl.when(step == 0)
            def _():
                rows[0:32, :] = rims[0][0:32, :].astype(jnp.float32)

        def oldest(at):
            reach = base + at - 30
            if begin > 0:
                return ids_ref[reach]
            return jnp.where(reach < 0, rim_first, ids_ref[jnp.maximum(reach, 0)])

        for at in range(0, tile, CHUNK):

            @pl.when(oldest(at) == ids_ref[base + at + CHUNK - 1])
            def _(at=at):
                total[at : at + CHUNK, :] = convolve(rows, at)

        def one_chunk(chunk, carry):
            at = pl.multiple_of(chunk * CHUNK, CHUNK)
            low, high = ids_ref[base + at], ids_ref[base + at + CHUNK - 1]

            @pl.when(oldest(at) != high)
            def _():
                total[pl.ds(at, CHUNK), :] = jnp.zeros((CHUNK, lanes), jnp.float32)

                def one_document(doc, carry):
                    first = begins(doc) - base - at + 2
                    last = begins(doc + 1) - base - at + 2
                    position = lax.broadcasted_iota(jnp.int32, masked.shape, 0)
                    masked[...] = jnp.where(
                        jnp.logical_and(position >= first, position < last),
                        rows[pl.ds(at, CHUNK + 32), :],
                        jnp.float32(0.0),
                    )
                    place = lax.broadcasted_iota(jnp.int32, (CHUNK, lanes), 0) + 32
                    inside = jnp.logical_and(place >= first, place < last)
                    total[pl.ds(at, CHUNK), :] += jnp.where(
                        inside, convolve(masked, 0), jnp.float32(0.0)
                    )
                    return carry

                lax.fori_loop(low, high + 1, one_document, 0)

            return carry

        lax.fori_loop(0, tile // CHUNK, one_chunk, 0)
        out_ref[step] = total[...].astype(out_ref.dtype)
        return carry

    lax.fori_loop(0, count, one_tile, 0)


def convolve_tokens(begin, count, tile, ids, gated, kernel, *rims):
    lanes = gated.shape[1]
    taps = kernel.shape[0]
    return pl.pallas_call(
        functools.partial(conv_kernel_body, begin),
        in_specs=[SMEM] + [VMEM] * (3 + len(rims)),
        out_specs=VMEM,
        scratch_shapes=[
            pltpu.VMEM((8 * taps, lanes), jnp.float32),
            pltpu.VMEM((tile + 32, lanes), jnp.float32),
            pltpu.VMEM((CHUNK + 32, lanes), jnp.float32),
            pltpu.VMEM((tile, lanes), jnp.float32),
        ],
        out_shape=jax.ShapeDtypeStruct((count, tile, lanes), jnp.bfloat16),
        compiler_params=params(12),
        name="conv_head" if begin == 0 else "conv_rest",
    )(ids, ids.reshape(-1, 128), gated, kernel, *rims)


def slots_body(capacity, routing_ref, spread_ref, first_ref, second_ref, choice_ref):
    count = routing_ref.shape[1]
    slots = spread_ref.shape[0]
    row = lax.broadcasted_iota(jnp.int32, (count, count), 0)
    column = lax.broadcasted_iota(jnp.int32, (count, count), 1)

    def ones(mask):
        return jnp.where(mask, jnp.float32(1.0), jnp.float32(0.0))

    sub = lax.broadcasted_iota(jnp.int32, (16, count), 0)
    one, two = routing_ref[0:1, :], routing_ref[1:2, :]
    named = jnp.logical_or(sub == one, sub == two)
    before = jnp.dot(
        ones(named).astype(jnp.bfloat16),
        ones(row < column).astype(jnp.bfloat16),
        preferred_element_type=jnp.float32,
    )
    slot = lax.broadcasted_iota(jnp.int32, (slots, count), 0)
    targets = []
    for chosen in (one, two):
        position = jnp.sum(jnp.where(sub == chosen, before, 0.0), axis=0, keepdims=True)
        targets.append(chosen * capacity + position.astype(jnp.int32))
    spread_ref[...] = ones(jnp.logical_or(slot == targets[0], slot == targets[1])).astype(
        jnp.bfloat16
    )

    def upright(line):
        turned = jnp.sum(
            jnp.where(row == column, line.astype(jnp.float32), 0.0), axis=1, keepdims=True
        )
        return turned.astype(jnp.int32)

    slot = lax.broadcasted_iota(jnp.int32, (count, slots), 1)
    for target, out in zip(targets, (first_ref, second_ref), strict=True):
        out[...] = ones(slot == upright(target)).astype(jnp.bfloat16)
    lane = lax.broadcasted_iota(jnp.int32, choice_ref.shape, 1)
    choice_ref[...] = jnp.where(lane == 0, upright(one), upright(two))


def stats_body(*refs):
    raw_refs, out_ref = refs[:-1], refs[-1]
    count, lanes = raw_refs[0].shape
    summed = jnp.zeros((count, lanes), jnp.float32)
    for raw in raw_refs:
        summed = summed + raw[...].astype(jnp.float32)
    average = jnp.sum(summed, axis=1, keepdims=True) * jnp.float32(1.0 / (lanes * len(raw_refs)))
    squares = jnp.zeros((count, lanes), jnp.float32)
    for raw in raw_refs:
        centered = raw[...].astype(jnp.float32) - average
        squares = squares + centered * centered
    squares = jnp.sum(squares, axis=1, keepdims=True)
    lane = lax.broadcasted_iota(jnp.int32, (count, lanes), 1)
    out_ref[...] = jnp.where(lane == 0, average, squares)


def activate_body(order, place_ref, mine_ref, other_ref, gain_ref, bias_ref, *refs):
    raw_refs, out_ref = refs[:-1], refs[-1]
    rows, lanes = raw_refs[0].shape
    count = rows // 2
    half = lanes * len(raw_refs)
    core = place_ref[1]
    for block in range(2):
        at = pl.ds(pl.multiple_of((core ^ block) * count, count), count)
        to = slice(block * count, block * count + count)
        mine, other = mine_ref[at, :], other_ref[at, :]
        average = (mine[:, 0:1] + other[:, 0:1]) * jnp.float32(0.5)
        apart = mine[:, 0:1] - other[:, 0:1]
        spread = mine[:, 1:2] + other[:, 1:2] + apart * apart * jnp.float32(half / 2)
        scale = lax.rsqrt(spread * jnp.float32(0.5 / half) + epsilon)
        for slot, raw in enumerate(raw_refs):
            part = 2 * (place_ref[0] ^ order[slot]) + core
            value = (raw[at, :].astype(jnp.float32) - average) * scale * gain_ref[part] + bias_ref[
                part
            ]
            out_ref[to, slot * lanes : slot * lanes + lanes] = jax.nn.silu(value).astype(
                jnp.bfloat16
            )


def partial_body(sources, place_ref, active_ref, *refs):
    pieces, (mine_ref, other_ref) = refs[:-2], refs[-2:]
    count = mine_ref.shape[1]
    u = place_ref[3]

    def half(source):
        ref = pieces[source[0]]
        return ref if len(source) == 1 else ref.at[source[1]]

    for number, halves in enumerate(sources):
        low, high = (half(source) for source in halves)
        nears, slots, depth, lanes = low.shape
        weight = jnp.concatenate(
            [
                jnp.concatenate(
                    [part[nth].reshape(slots * depth, lanes) for part in (low, high)], axis=0
                )
                for nth in range(nears)
            ],
            axis=1,
        )
        product = jnp.dot(active_ref[...], weight, preferred_element_type=jnp.float32)
        for nth, near in enumerate(NEAR):
            piece = product[:, nth * lanes : nth * lanes + lanes]
            to = pl.ds(pl.multiple_of((u ^ near) * lanes, lanes), lanes)
            mine_ref[number, :, to] = piece[:count]
            other_ref[number, :, to] = piece[count:].astype(other_ref.dtype)


def partial_products(sources, place, active, pieces):
    rows = active.shape[0]
    shape = (len(sources), rows // 2, 512)
    return pl.pallas_call(
        functools.partial(partial_body, sources),
        in_specs=[SMEM] + [VMEM] * (1 + len(pieces)),
        out_specs=[VMEM] * 2,
        out_shape=[
            jax.ShapeDtypeStruct(shape, jnp.float32),
            jax.ShapeDtypeStruct(shape, jnp.bfloat16),
        ],
        compiler_params=params(16),
    )(place, active, *pieces)


def state_body(
    groups,
    experts,
    place_ref,
    mine_1_ref,
    other_1_ref,
    mine_2_ref,
    other_2_ref,
    residual_ref,
    gain_moe_ref,
    router_ref,
    choice_ref,
    spread_ref,
    state_ref,
    mix_ref,
    outgoing_ref,
    projected_ref,
):
    group = mine_1_ref.shape[2]
    mine = [ref[part] for ref in (mine_1_ref, mine_2_ref) for part in range(2)]
    other = [ref[part] for ref in (other_1_ref, other_2_ref) for part in range(2)]
    for coordinate, blocks in ((2, mine), (3, other)):
        for far, block in zip(NEAR, blocks, strict=True):
            at = pl.ds(pl.multiple_of((place_ref[coordinate] ^ far) * group, group), group)
            held = residual_ref if coordinate == 2 else projected_ref
            projected_ref[:, at] = held[:, at].astype(jnp.float32) + block.astype(jnp.float32)
    projected = projected_ref[...]
    state = projected.astype(jnp.bfloat16)
    state_ref[...] = state
    state = state.astype(jnp.float32)
    power = jnp.mean(state * state, axis=1, keepdims=True)
    normed = (state * lax.rsqrt(power + epsilon) * gain_moe_ref[...]).astype(jnp.bfloat16)
    outgoing_ref[...] = jnp.dot(
        spread_ref[...], normed, preferred_element_type=jnp.float32
    ).astype(jnp.bfloat16)
    logits = lax.dot_general(
        normed, router_ref[...], (((1,), (1,)), ((), ())), preferred_element_type=jnp.float32
    )
    lane = lax.broadcasted_iota(jnp.int32, logits.shape, 1)
    one, two = choice_ref[:, 0:1], choice_ref[:, 1:2]
    group = one // (experts // groups)

    def pick(mask, array):
        return jnp.sum(jnp.where(mask, array, jnp.float32(0.0)), axis=1, keepdims=True)

    raised = jnp.exp(logits)
    in_groups = jnp.logical_and(lane >= experts, lane < experts + groups)
    group_prob = pick(lane == experts + group, raised) / pick(in_groups, raised)
    first = jnp.exp(pick(lane == one, logits))
    second = jnp.exp(pick(lane == two, logits))
    both = first + second
    mix_ref[...] = jnp.where(
        lane == 0, group_prob * first / both, jnp.where(lane == 1, group_prob * second / both, 0.0)
    )


def experts_body(rows_ref, gate_ref, up_ref, down_ref, out_ref):
    rows = rows_ref[...]
    gate = jnp.dot(rows, gate_ref[...], preferred_element_type=jnp.float32)
    up = jnp.dot(rows, up_ref[...], preferred_element_type=jnp.float32)
    hidden = (jax.nn.silu(gate) * up).astype(jnp.bfloat16)
    out_ref[...] = jnp.dot(hidden, down_ref[...], preferred_element_type=jnp.float32).astype(
        jnp.bfloat16
    )


def mix_body(state_ref, first_ref, second_ref, mix_ref, returned_ref, out_ref):
    returned = returned_ref[...]
    first = jnp.dot(first_ref[...], returned, preferred_element_type=jnp.float32)
    second = jnp.dot(second_ref[...], returned, preferred_element_type=jnp.float32)
    mixture = mix_ref[:, 0:1] * first + mix_ref[:, 1:2] * second
    out_ref[...] = (state_ref[...].astype(jnp.float32) + mixture).astype(jnp.bfloat16)


def swap(array, dz=0, dc=0):
    flip = dz * 2 + dc
    return lax.ppermute(array, ("sp", "tp"), [(i, i ^ flip) for i in range(256)])


def cross(array, by, turn):
    pairs = [(i, i ^ (by * (16 if (i & 1) == turn else 64))) for i in range(256)]
    return lax.ppermute(array, ("sp", "tp"), pairs)


def shifted(array, axis, by):
    count = lax.axis_size(axis)
    pairs = [(i, i + by) for i in range(count) if 0 <= i + by < count]
    return lax.ppermute(array, axis, pairs)


def body(
    conv_value,
    conv_gate,
    doc_ids,
    conv_kernel,
    norm_gain_conv,
    norm_bias_conv,
    proj_weight,
    residual,
    norm_gain_moe,
    group_router,
    expert_router,
    routing,
    expert_gate_w,
    expert_up_w,
    expert_down_w,
):
    tokens, lanes = conv_value.shape
    count, width = residual.shape
    groups, experts = group_router.shape[1], expert_router.shape[1]
    slots = 2 * count
    capacity = slots // experts

    sp, tp = lax.axis_index("sp"), lax.axis_index("tp")
    z, core, y, x = tp >> 1, tp & 1, sp >> 2, sp & 3
    u, v = jnp.where(core == 0, x, y), jnp.where(core == 0, y, x)
    place = jnp.stack([z, core, v, u]).astype(jnp.int32)

    gated = (
        conv_value.astype(jnp.float32) * jax.nn.sigmoid(conv_gate.astype(jnp.float32))
    ).astype(jnp.bfloat16)
    tail = slice(tokens - 32, tokens)
    tail_ids = jnp.broadcast_to(doc_ids[tail][:, None], (32, lanes)).astype(jnp.bfloat16)
    message = jnp.concatenate([gated[tail], tail_ids], axis=0)
    came = shifted(message, "sp", 1)

    held = lax.dynamic_slice_in_dim(proj_weight, (v * 4 + u) * 128, 128, axis=1)[None]
    for bit in (4, 2, 1):
        other = swap(held, dz=bit)
        held = jnp.concatenate([held, other], axis=0)
    near = [held]
    for d in NEAR[1:]:
        near.append(cross(held, d, 0))
    low, high = (jnp.stack([part[at : at + 4] for part in near]) for at in (0, 4))
    low_1 = cross(low, 1, 1)
    high_3 = cross(high, 3, 1)
    low_32 = cross(jnp.stack([low, low_1]), 3, 1)
    high_12 = cross(jnp.stack([high, high_3]), 1, 1)

    tile = 2 * count
    rest = convolve_tokens(4, 4, tile, doc_ids, gated, conv_kernel)
    head = convolve_tokens(0, 4, tile, doc_ids, gated, conv_kernel, came)
    convolved = lax.optimization_barrier(jnp.concatenate([head, rest], axis=0))
    raw = []
    for d in ORDER:
        part = lax.dynamic_index_in_dim(convolved, z ^ d, 0, keepdims=False)
        raw.append(swap(part, dz=d) if d else part)

    spread, first_pick, second_pick, choice = pl.pallas_call(
        functools.partial(slots_body, capacity),
        in_specs=[VMEM],
        out_specs=[VMEM] * 4,
        out_shape=[
            jax.ShapeDtypeStruct((slots, count), jnp.bfloat16),
            jax.ShapeDtypeStruct((count, slots), jnp.bfloat16),
            jax.ShapeDtypeStruct((count, slots), jnp.bfloat16),
            jax.ShapeDtypeStruct((count, 128), jnp.int32),
        ],
        compiler_params=params(8),
        name="slots",
    )(routing.T)
    routers = jnp.concatenate(
        [
            expert_router.T,
            group_router.T,
            jnp.zeros((32 - experts - groups, width), jnp.bfloat16),
        ],
        axis=0,
    )
    rows = 2 * count
    mine = pl.pallas_call(
        stats_body,
        in_specs=[VMEM] * 8,
        out_specs=VMEM,
        out_shape=jax.ShapeDtypeStruct((rows, lanes), jnp.float32),
        compiler_params=params(8),
        name="stats",
    )(*raw)
    other = swap(mine, dc=1)
    active = pl.pallas_call(
        functools.partial(activate_body, ORDER),
        in_specs=[SMEM] + [VMEM] * 12,
        out_specs=VMEM,
        out_shape=jax.ShapeDtypeStruct((rows, 8 * lanes), jnp.bfloat16),
        compiler_params=params(8),
        name="activate",
    )(
        place,
        mine,
        other,
        norm_gain_conv.reshape(-1, 1, lanes),
        norm_bias_conv.reshape(-1, 1, lanes),
        *raw,
    )
    kept_1, given_1 = partial_products(
        (((0,), (1,)), ((2,), (3, 0))), place, active, (low, high, low_1, high_12)
    )
    kept_2, given_2 = partial_products(
        (((0, 0), (1,)), ((0, 1), (2, 1))), place, active, (low_32, high_3, high_12)
    )
    taken_1 = swap(given_1, dc=1)
    taken_2 = swap(given_2, dc=1)
    state, mix, outgoing = pl.pallas_call(
        functools.partial(state_body, groups, experts),
        in_specs=[SMEM] + [VMEM] * 9,
        out_specs=[VMEM] * 3,
        scratch_shapes=[pltpu.VMEM((count, width), jnp.float32)],
        out_shape=[
            jax.ShapeDtypeStruct((count, width), jnp.bfloat16),
            jax.ShapeDtypeStruct((count, 32), jnp.float32),
            jax.ShapeDtypeStruct((slots, width), jnp.bfloat16),
        ],
        compiler_params=params(24),
        name="state",
    )(
        place,
        kept_1,
        taken_1,
        kept_2,
        taken_2,
        residual,
        norm_gain_moe[None, :],
        routers,
        choice,
        spread,
    )

    def exchanged(rows):
        blocks = rows.reshape(experts, capacity, width)
        return lax.all_to_all(blocks, "sp", split_axis=0, concat_axis=0, tiled=True).reshape(
            slots, width
        )

    result = pl.pallas_call(
        experts_body,
        in_specs=[VMEM] * 4,
        out_specs=VMEM,
        out_shape=jax.ShapeDtypeStruct((slots, width), jnp.bfloat16),
        compiler_params=params(20),
        name="experts",
    )(exchanged(outgoing), expert_gate_w[0], expert_up_w[0], expert_down_w[0])
    return pl.pallas_call(
        mix_body,
        in_specs=[VMEM] * 5,
        out_specs=VMEM,
        out_shape=jax.ShapeDtypeStruct((count, width), jnp.bfloat16),
        compiler_params=params(16),
        name="mix",
    )(state, first_pick, second_pick, mix, exchanged(result))


def solution(mesh):
    placed = (
        P("sp", "tp"),
        P("sp", "tp"),
        P("sp"),
        P(None, "tp"),
        P(),
        P(),
        P("tp", None),
        P(("sp", "tp"), None),
        P(),
        P(),
        P(),
        P(("sp", "tp"), None),
        P("sp", None, None),
        P("sp", None, None),
        P("sp", None, None),
    )

    return jax.shard_map(
        body, mesh=mesh, in_specs=placed, out_specs=P(("sp", "tp"), None), check_vma=False
    )
```
